32 devices in a mesh: sp: 16 (over z, y, x), tp: 2 (over core).
Axes of the slice: x: 2, y: 2, z: 4, core: 2. Of those that a mesh axis runs over, the one named last changes fastest.
Arguments:
- tokens: bfloat16 [2048, 2048], P('sp', 'tp'), may hold values from -6 to 6
- pre_gain: float32 [2048], replicated, may hold values from 0.1 to 1.9
- w_query_stick: bfloat16 [2048, 1024], P(None, 'tp'), may hold values from -0.125 to 0.125
- w_key_stick: bfloat16 [2048, 1024], P(None, 'tp'), may hold values from -0.125 to 0.125
- w_value_stick: bfloat16 [2048, 1024], P(None, 'tp'), may hold values from -2 to 2, as said below
- w_query_window: bfloat16 [2048, 1024], P(None, 'tp'), may hold values from -20 to 20, as said below
- w_key_window: bfloat16 [2048, 512], P(None, 'tp'), may hold values from -1 to 1, as said below
- w_value_window: bfloat16 [2048, 512], P(None, 'tp'), may hold values from -2 to 2, as said below
- stick_bias: float32 [16], P('tp'), may hold values from -14 to -3
- sinks: float32 [16], P('tp'), may hold values from 2 to 6
- stick_gain: float32 [1024], P('tp'), may hold values from 0.1 to 1.9
- window_gain: float32 [1024], P('tp'), may hold values from 0.1 to 1.9
- w_out_stick: bfloat16 [1024, 2048], P('tp'), may hold values from -0.125 to 0.125
- w_out_window: bfloat16 [1024, 2048], P('tp'), may hold values from -0.125 to 0.125
- post_gain: float32 [2048], replicated, may hold values from 0.1 to 1.9
Outputs:
- layer_out: bfloat16 [2048, 2048], P(('sp', 'tp'))
The draws below stay inside these ranges and needn't reach their ends.
Inputs may be any that keep to these rules, and one draw needn't show every extreme that they name: `w_key_window`: key weights of the windowed heads. `w_query_window`: query weights of the windowed heads. `w_value_stick`: value weights of the stick-breaking heads. `w_value_window`: value weights of the windowed heads.
All inputs are finite; a program needn't handle non-finite values.
Results may differ from the reference program's by a relative error of at most 0.018.
Values may be sent and summed in bfloat16 or wider, within the bound.
A program may use at most 64 MiB of HBM per device.

```python
import jax
import jax.numpy as jnp
from jax import lax

D = 2048
HEAD_DIM = 64
SB_HEADS = 16
SW_KV_HEADS = 8
GROUP = 2
WINDOW = 128
TOK_DEV = 128
TOKENS = 2048
SW_HEADS = 16
SB_WIDTH = 1024
SW_WIDTH = 1024


def clipped_normal(key, shape):
    return jnp.clip(jax.random.normal(key, shape, jnp.float32), -4.0, 4.0)


def window_pair(key):
    salted = jax.random.fold_in(key, 17)
    keys_w = clipped_normal(jax.random.fold_in(salted, 1), (D, SW_KV_HEADS * HEAD_DIM)) * D ** (-0.5)
    queries_w = clipped_normal(jax.random.fold_in(salted, 2), (D, SW_HEADS * HEAD_DIM)) * D ** (-0.5)
    return (keys_w, queries_w)


def draw_w_key_window(key, part):
    return window_pair(key)[0].astype(jnp.bfloat16)


def draw_w_query_window(key, part):
    keys_w, queries_w = window_pair(key)
    return queries_w.astype(jnp.bfloat16)


def scaled_values(key, salt, head_count):
    salted = jax.random.fold_in(key, salt)
    head_scale = jnp.exp(jax.random.uniform(jax.random.fold_in(salted, 1), (head_count,), jnp.float32, -1.2, 1.2))
    normals = clipped_normal(jax.random.fold_in(salted, 2), (D, head_count * HEAD_DIM)) * D ** (-0.5)
    return normals * jnp.repeat(head_scale, HEAD_DIM)[None, :]


def draw_w_value_stick(key, part):
    return scaled_values(key, 23, SB_HEADS).astype(jnp.bfloat16)


def draw_w_value_window(key, part):
    return scaled_values(key, 31, SW_KV_HEADS).astype(jnp.bfloat16)


def draw_stick_bias(key, part):
    salted = jax.random.fold_in(key, 29)
    slow_bias = -jnp.log(TOKENS * 1.0) - jax.random.uniform(jax.random.fold_in(salted, 1), (SB_HEADS,), jnp.float32, 0.0, 1.0)
    fast_bias = jax.random.uniform(jax.random.fold_in(salted, 2), (SB_HEADS,), jnp.float32, -4.0, -3.5)
    chosen = jax.random.permutation(jax.random.fold_in(salted, 3), SB_HEADS) < SB_HEADS // 2
    return jnp.where(chosen, slow_bias, fast_bias)


def steps_of(own_key, shape, split, smallest, high):
    def one(position, blocks):
        heights = jax.random.uniform(jax.random.fold_in(jax.random.fold_in(own_key, 6), position), (blocks,), jnp.float32, smallest / len(split), high / len(split))
        return jnp.repeat(jnp.exp(heights), shape[position] // blocks).reshape((-1,) + (1,) * (len(shape) - position - 1))

    level = one(*split[0])
    for cut in split[1:]:
        level = level * one(*cut)
    return level


def scatter_about(own_key, shape, width, most, split=(), held_as=jnp.bfloat16):
    values = width * jax.random.normal(own_key, shape, jnp.float32)
    if split:
        values = values * steps_of(own_key, shape, split, -0.22, 0.18)
    return jnp.clip(values, -most, most).astype(held_as)


def setup_inputs(seed: int = 0) -> dict:
    key_of = jax.random.split(jax.random.key(seed), 16)
    return {
        "tokens": scatter_about(key_of[0], (TOKENS, D), 1.0, 6.0, ((0, 16), (1, 2))),
        "pre_gain": jnp.clip(1.0 + 0.18 * jax.random.normal(key_of[1], (D,), jnp.float32), 0.1, 1.9),
        "w_query_stick": scatter_about(key_of[2], (D, SB_WIDTH), D ** -0.5, 0.125, ((1, 2),)),
        "w_key_stick": scatter_about(key_of[3], (D, SB_WIDTH), D ** -0.5, 0.125, ((1, 2),)),
        "w_value_stick": draw_w_value_stick(jax.random.fold_in(key_of[15], 71), 0),
        "w_query_window": draw_w_query_window(jax.random.fold_in(key_of[15], 71), 0),
        "w_key_window": draw_w_key_window(jax.random.fold_in(key_of[15], 71), 0),
        "w_value_window": draw_w_value_window(jax.random.fold_in(key_of[15], 71), 0),
        "stick_bias": draw_stick_bias(jax.random.fold_in(key_of[15], 71), 0),
        "sinks": jnp.clip(2.0 + 4.0 * jax.random.uniform(key_of[9], (SW_HEADS,), jnp.float32) ** steps_of(key_of[9], (SW_HEADS,), ((0, 2),), -0.2, 0.2), 2.0, 6.0),
        "stick_gain": jnp.clip(1.0 + 0.18 * jax.random.normal(key_of[10], (SB_WIDTH,), jnp.float32), 0.1, 1.9),
        "window_gain": jnp.clip(1.0 + 0.18 * jax.random.normal(key_of[11], (SW_WIDTH,), jnp.float32), 0.1, 1.9),
        "w_out_stick": scatter_about(key_of[12], (SB_WIDTH, D), (SB_WIDTH + SW_WIDTH) ** -0.5, 0.125, ((0, 2),)),
        "w_out_window": scatter_about(key_of[13], (SW_WIDTH, D), (SB_WIDTH + SW_WIDTH) ** -0.5, 0.125, ((0, 2),)),
        "post_gain": jnp.clip(1.0 + 0.18 * jax.random.normal(key_of[14], (D,), jnp.float32), 0.1, 1.9),
    }


epsilon = 1e-06

def rounded(values):
    return lax.optimization_barrier(values.astype(jnp.bfloat16)).astype(jnp.float32)

def norm_rows(values, gain):
    stats = lax.optimization_barrier(jnp.mean(values * values, axis=-1, keepdims=True))
    return values * lax.rsqrt(stats + epsilon) * gain

def stick_attention(queries, key_rows, values, stick_bias):
    blocks = TOKENS // TOK_DEV
    q_blocks = queries.reshape(blocks, TOK_DEV, SB_HEADS, HEAD_DIM).astype(jnp.float32)
    k_blocks = key_rows.reshape(blocks, TOK_DEV, SB_HEADS, HEAD_DIM).astype(jnp.float32)
    v_blocks = values.reshape(blocks, TOK_DEV, SB_HEADS, HEAD_DIM).astype(jnp.float32)
    offsets = jnp.arange(TOK_DEV, dtype=jnp.int32)
    scaling = HEAD_DIM ** (-0.5)

    def one_query(block_args):
        q_blk, q_index = block_args
        q_pos = q_index * TOK_DEV + offsets

        def key_step(carried, inputs):
            result, logsum = carried
            k_blk, v_blk, k_index = inputs
            k_pos = k_index * TOK_DEV + offsets
            before = (k_pos[None, :] < q_pos[:, None])[None]
            scores = jnp.einsum('thd,shd->hts', q_blk, k_blk) * scaling + stick_bias[:, None, None]
            log_keep = jnp.where(before, jax.nn.log_sigmoid(-scores), 0.0)
            suffix = lax.cumsum(log_keep, axis=2, reverse=True) - log_keep
            stick_weights = jnp.where(before, jnp.exp(jax.nn.log_sigmoid(scores) + suffix + logsum[:, :, None]), 0.0)
            stick_weights = rounded(stick_weights)
            result = result + jnp.einsum('hts,shd->htd', stick_weights, v_blk)
            logsum = logsum + lax.optimization_barrier(jnp.sum(log_keep, axis=2))
            return ((result, logsum), None)
        initial = (jnp.zeros((SB_HEADS, TOK_DEV, HEAD_DIM), jnp.float32), jnp.zeros((SB_HEADS, TOK_DEV), jnp.float32))
        (result, _), _ = lax.scan(key_step, initial, (k_blocks, v_blocks, jnp.arange(blocks, dtype=jnp.int32)), reverse=True)
        return result.transpose(1, 0, 2)
    outputs = lax.map(one_query, (q_blocks, jnp.arange(blocks, dtype=jnp.int32)))
    return outputs.reshape(TOKENS, SB_WIDTH).astype(jnp.bfloat16)

def window_attention(queries, key_rows, values, sinks):
    block_count = TOKENS // WINDOW
    q_blocks = queries.reshape(block_count, WINDOW, SW_KV_HEADS, GROUP, HEAD_DIM).astype(jnp.float32)
    k_heads = key_rows.reshape(block_count, WINDOW, SW_KV_HEADS, HEAD_DIM).astype(jnp.float32)
    v_heads = values.reshape(block_count, WINDOW, SW_KV_HEADS, HEAD_DIM).astype(jnp.float32)
    zero_block = jnp.zeros((1, WINDOW, SW_KV_HEADS, HEAD_DIM), jnp.float32)
    k_band = jnp.concatenate([jnp.concatenate([zero_block, k_heads[:-1]], axis=0), k_heads], axis=1)
    v_band = jnp.concatenate([jnp.concatenate([zero_block, v_heads[:-1]], axis=0), v_heads], axis=1)
    logits = jnp.einsum('nqhgd,nchd->nhgqc', q_blocks, k_band) * HEAD_DIM ** (-0.5)
    query_offs = jnp.arange(WINDOW, dtype=jnp.int32)[:, None]
    key_offs = jnp.arange(2 * WINDOW, dtype=jnp.int32)[None, :]
    distance = query_offs + WINDOW - key_offs
    key_pos = jnp.arange(block_count, dtype=jnp.int32)[:, None] * WINDOW - WINDOW + key_offs
    usable = ((distance >= 0) & (distance < WINDOW))[None] & (key_pos >= 0)[:, None, :]
    logits = jnp.where(usable[:, None, None], logits, -jnp.inf)
    sink_logit = sinks.reshape(SW_KV_HEADS, GROUP)[None, :, :, None, None]
    row_top = jnp.maximum(lax.optimization_barrier(jnp.max(logits, axis=-1, keepdims=True)), sink_logit)
    weights_exp = jnp.exp(logits - row_top)
    normalizer = lax.optimization_barrier(jnp.sum(weights_exp, axis=-1, keepdims=True)) + jnp.exp(sink_logit - row_top)
    window_weights = rounded(weights_exp / normalizer)
    result = jnp.einsum('nhgqc,nchd->nqhgd', window_weights, v_band)
    return result.reshape(TOKENS, SW_WIDTH).astype(jnp.bfloat16)

def reference(tokens, pre_gain, w_query_stick, w_key_stick, w_value_stick, w_query_window, w_key_window, w_value_window, stick_bias, sinks, stick_gain, window_gain, w_out_stick, w_out_window, post_gain):
    normed = norm_rows(tokens.astype(jnp.float32), pre_gain).astype(jnp.bfloat16)

    def project(weight):
        return jnp.dot(normed, weight, preferred_element_type=jnp.float32).astype(jnp.bfloat16)
    stick_out = stick_attention(project(w_query_stick), project(w_key_stick), project(w_value_stick), stick_bias)
    window_out = window_attention(project(w_query_window), project(w_key_window), project(w_value_window), sinks)
    stick_normed = norm_rows(stick_out.astype(jnp.float32), stick_gain).astype(jnp.bfloat16)
    window_normed = norm_rows(window_out.astype(jnp.float32), window_gain).astype(jnp.bfloat16)
    combined = jnp.dot(stick_normed, w_out_stick, preferred_element_type=jnp.float32)
    combined = combined + jnp.dot(window_normed, w_out_window, preferred_element_type=jnp.float32)
    combined = rounded(combined)
    return norm_rows(combined, post_gain).astype(jnp.bfloat16)
```

```python
import functools

import jax
import jax.numpy as jnp
from jax import lax
from jax.experimental import pallas as pl
from jax.experimental.pallas import tpu as pltpu
from jax.sharding import PartitionSpec as P

HEAD_DIM = 64
GROUP = 2
WINDOW = 128
EPS = 1e-06
LOG2E = 1.4426950408889634
MESH = pl.DeviceIdType.MESH


class Phases:
    def __init__(self):
        self.scope = None

    def __call__(self, name):
        if self.scope is not None:
            self.scope.__exit__(None, None, None)
            self.scope = None
        if name:
            self.scope = jax.named_scope(name)
            self.scope.__enter__()


def dot(a, b):
    return jnp.dot(a, b, preferred_element_type=jnp.float32)


def dot_t(a, b):
    return lax.dot_general(a, b, (((1,), (1,)), ((), ())), preferred_element_type=jnp.float32)


def chosen(at, table):
    value = jnp.int32(table[0])
    for n in range(1, len(table)):
        if table[n] != table[0]:
            value = jnp.where(at == n, jnp.int32(table[n]), value)
    return value


def kernel(
    n_sp,
    tokens, pre_gain_in, wqs, wks, wvs, wqw, wkw, wvw, bias_in, sinks_in, sgain_in, wgain_in, wos, wow,
    post_gain_in, out,
    pre_gain, bias, sinks, sgain, wgain, post_gain, x, bias_buf, xg, vqs, vks, vvs, vqw, vkw, vvw, vos, vow,
    proj, kv_send, kv_all, q_pad, part, mass,
    qw, kvw, kvw_prev, w_out_buf, o_send, o_recv, s_out_buf,
    sq_send, sq_recv, total_w, comb, c_send, c_recv,
    w_sem, small_sem, tok_sem, x_ss, x_rs, b_ss, b_rs, kv_ss, kv_rs, f_ss, f_rs,
    p_ss, p_rs, o_ss, o_rs, sq_ss, sq_rs, c_ss, c_rs,
):
    bf = jnp.bfloat16
    f32 = jnp.float32
    s = lax.axis_index("sp")
    t = lax.axis_index("tp")
    other = 1 - t
    rows, feat_half = tokens.shape
    feats = 2 * feat_half
    half = rows // 2
    quarter = half // 2
    hd = HEAD_DIM
    heads = wqs.shape[1] // hd
    kv_heads = wkw.shape[1] // hd
    sw = wqs.shape[1]
    n_chunks = n_sp // 4
    ph = Phases()
    ph("a_entry")

    tok_load = pltpu.make_async_copy(tokens, x.at[0], tok_sem)
    tok_load.start()
    smalls = [
        pltpu.make_async_copy(src, dst, small_sem.at[n])
        for n, (src, dst) in enumerate(
            [(bias_in, bias), (pre_gain_in, pre_gain), (sinks_in, sinks), (sgain_in, sgain),
             (wgain_in, wgain), (post_gain_in, post_gain)]
        )
    ]
    for load in smalls:
        load.start()

    barrier = pltpu.get_barrier_semaphore()
    me = s * 2 + t

    def greet(k, carry):
        peer = lax.rem(me + k, 2 * n_sp)
        pl.semaphore_signal(
            barrier, inc=1, device_id={"sp": peer // 2, "tp": lax.rem(peer, 2)}, device_id_type=MESH
        )
        return carry

    lax.fori_loop(1, 2 * n_sp, greet, 0)

    own_rows = pl.ds(pl.multiple_of(t * feat_half, feat_half), feat_half)
    other_rows = pl.ds(pl.multiple_of(other * feat_half, feat_half), feat_half)
    loads = {}
    for n, (name, src, dst) in enumerate(
        [("ks", wks, vks), ("vs", wvs, vvs), ("qs", wqs, vqs), ("kw", wkw, vkw), ("vw", wvw, vvw), ("qw", wqw, vqw)]
    ):
        loads[name] = [
            pltpu.make_async_copy(src.at[own_rows], dst.at[0], w_sem.at[2 * n]),
            pltpu.make_async_copy(src.at[other_rows], dst.at[1], w_sem.at[2 * n + 1]),
        ]
    l_ow = pltpu.make_async_copy(wow, vow, w_sem.at[12])
    l_os = pltpu.make_async_copy(wos, vos, w_sem.at[13])

    ph("b_tokwait")
    tok_load.wait()
    for load in smalls:
        load.wait()
    for part_of in range(2):
        for name in ("ks", "vs", "qs"):
            loads[name][part_of].start()

    row_id = lax.broadcasted_iota(jnp.int32, (heads, 128), 0)
    bias_rows = jnp.zeros((heads, 128), f32)
    for i in range(heads):
        bias_rows = jnp.where(row_id == i, bias[i] * LOG2E, bias_rows)
    bias_buf[t] = bias_rows

    ph("c_gain")
    gain = pre_gain[...].reshape(1, feats)
    gains = [
        jnp.where(t == 0, gain[:, :feat_half], gain[:, feat_half:]),
        jnp.where(t == 0, gain[:, feat_half:], gain[:, :feat_half]),
    ]

    def scaled(n):
        value = x[n].astype(f32)
        xg[n] = (value * gains[n]).astype(bf)
        return jnp.sum(value * value, axis=1, keepdims=True)

    squares = scaled(0)

    ph("d_barrier")
    pl.semaphore_wait(barrier, 2 * n_sp - 1)

    def to_partner(src, dst, ss, rs):
        return pltpu.make_async_remote_copy(
            src_ref=src, dst_ref=dst, send_sem=ss, recv_sem=rs,
            device_id={"sp": s, "tp": other}, device_id_type=MESH,
        )

    x_copy = to_partner(x.at[0], x.at[1], x_ss, x_rs)
    b_copy = to_partner(bias_buf.at[t], bias_buf.at[t], b_ss, b_rs)
    x_copy.start()
    b_copy.start()

    ph("e_own")
    for n, (name, w) in enumerate([("ks", vks), ("vs", vvs), ("qs", vqs)]):
        loads[name][0].wait()
        proj[n] = dot(xg[0], w[0])
    for name in ("kw", "vw", "qw"):
        for load in loads[name]:
            load.start()
    ph("f_xwait")
    x_copy.wait_recv()
    ph("g_kv")
    inv = lax.rsqrt((squares + scaled(1)) * (1.0 / feats) + EPS)
    loads["ks"][1].wait()
    keys = (proj[0] + dot(xg[1], vks[1])) * inv
    loads["vs"][1].wait()
    values = (proj[1] + dot(xg[1], vvs[1])) * inv
    for i in range(heads):
        cols = slice(i * hd, (i + 1) * hd)
        packed = jnp.concatenate([keys[:, cols], values[:, cols]], axis=1).astype(bf)
        kv_send[i, :, :half] = packed.reshape(2, half, 2 * hd)
    ph("h_q")
    loads["qs"][1].wait()
    queries = (proj[2] + dot(xg[1], vqs[1])) * inv
    for i in range(heads):
        cols = slice(i * hd, (i + 1) * hd)
        for u in range(2):
            top = queries[u * half : u * half + quarter, cols]
            low = queries[u * half + quarter : (u + 1) * half, cols]
            kv_send[i, u, half:] = jnp.concatenate([top, low], axis=1).astype(bf)

    ph("i_scatter")
    zone = s // 4
    owner = lax.rem(s, 2)
    slot = s // 2

    def dest_order(n):
        by_zone = []
        for z in range(n_chunks):
            order = sorted(range(heads), key=lambda i: (SIGN * abs(i // 2 - z), i // 2, i))
            by_zone.append(order[n])
        return chosen(zone, by_zone)

    for n in range(heads):
        i = dest_order(n)
        chip = 2 * i + t
        for u in range(2):
            is_self = jnp.logical_and(chip == s, u == t)

            @pl.when(is_self)
            def _():
                pltpu.make_async_copy(kv_send.at[i, u], kv_all.at[s, u], kv_rs.at[s]).start()

            @pl.when(jnp.logical_not(is_self))
            def _():
                pltpu.make_async_remote_copy(
                    src_ref=kv_send.at[i, u], dst_ref=kv_all.at[s, u], send_sem=kv_ss.at[i, u],
                    recv_sem=kv_rs.at[s], device_id={"sp": chip, "tp": u}, device_id_type=MESH,
                ).start()

    ph("j_wproj")
    l_ow.start()
    l_os.start()
    for load in loads["kw"] + loads["vw"]:
        load.wait()
    kvw[:, : kv_heads * hd] = ((dot(xg[0], vkw[0]) + dot(xg[1], vkw[1])) * inv).astype(bf)
    kvw[:, kv_heads * hd :] = ((dot(xg[0], vvw[0]) + dot(xg[1], vvw[1])) * inv).astype(bf)
    prev_copy = lambda to: pltpu.make_async_remote_copy(
        src_ref=kvw, dst_ref=kvw_prev, send_sem=p_ss, recv_sem=p_rs,
        device_id={"sp": to, "tp": t}, device_id_type=MESH,
    )

    @pl.when(s < n_sp - 1)
    def _():
        prev_copy(s + 1).start()

    for load in loads["qw"]:
        load.wait()
    qw[...] = ((dot(xg[0], vqw[0]) + dot(xg[1], vqw[1])) * inv).astype(bf)

    ph("k_misc")

    def forward(src):
        pltpu.make_async_remote_copy(
            src_ref=kv_send.at[0, 0], dst_ref=kv_all.at[src, t], send_sem=kv_ss.at[0, 0],
            recv_sem=kv_rs.at[src], device_id={"sp": s, "tp": other}, device_id_type=MESH,
        ).wait_recv()
        to_partner(kv_all.at[src, t, :half], kv_all.at[src, t, :half], f_ss.at[src], f_rs.at[src]).start()

    def forward_arrived(k):
        to_partner(kv_all.at[k, other, :half], kv_all.at[k, other, :half], f_ss.at[k], f_rs.at[k]).wait_recv()

    def take_q(k):
        slab = kv_all[k, t, half:].astype(f32)
        zero = jnp.zeros((quarter, hd), f32)
        both = jnp.concatenate(
            [
                jnp.concatenate([slab[:, :hd], zero], axis=1),
                jnp.concatenate([slab[:, hd:], zero], axis=1),
            ],
            axis=0,
        )
        q_pad[pl.ds(pl.multiple_of(k * half, half), half), :] = both.astype(bf)

    b_copy.wait_recv()
    head_bias = bias_buf[owner, pl.ds(slot, 1), :][:, :1]

    kt = 2 * rows
    chunk = 4 * half
    later = (
        lax.broadcasted_iota(jnp.int32, (kt, kt), 0) > lax.broadcasted_iota(jnp.int32, (kt, kt), 1)
    ).astype(bf)
    low = chunk // 2
    row = lax.broadcasted_iota(jnp.int32, (low, kt), 0)
    lane = lax.broadcasted_iota(jnp.int32, (low, kt), 1)
    before = lane < (row // half) * rows + t * half + lax.rem(row, half)
    scale = LOG2E * hd**-0.5

    def tile(qs, kv, masked):
        z = dot_t(qs, kv) * scale + head_bias
        pos = jnp.maximum(z, 0.0)
        neg = z - pos
        soft = jnp.log2(1.0 + jnp.exp2(neg - pos))
        drop = pos + soft
        hold = neg - soft
        if masked:
            n = before.shape[0]
            drop_top = jnp.where(before, drop[:n], 0.0)
            hold_top = jnp.where(before, hold[:n], -jnp.inf)
            drop = drop_top if n == drop.shape[0] else jnp.concatenate([drop_top, drop[n:]], axis=0)
            hold = hold_top if n == hold.shape[0] else jnp.concatenate([hold_top, hold[n:]], axis=0)
        suffix = dot(drop.astype(bf), later)
        total = jnp.broadcast_to(suffix[:, :1] + drop[:, :1], (drop.shape[0], 2 * hd))
        res = dot(jnp.exp2(hold - suffix).astype(bf), kv)
        return res, total

    def keys_of(kc, n):
        return kv_all[pl.ds(kc * 4 + 2 * n, 2), :, :half].reshape(kt, 2 * hd)

    def diagonal(c):
        qs = q_pad[pl.ds(pl.multiple_of(c * chunk, chunk), chunk), :]
        res1, total1 = tile(qs[low:], keys_of(c, 1), True)
        res0, total0 = tile(qs, keys_of(c, 0), True)
        part[c, c, :low] = res0[:low]
        mass[c, c, :low] = total0[:low]
        part[c, c, low:] = res1 + jnp.exp2(-total1) * res0[low:]
        mass[c, c, low:] = total0[low:] + total1

    def beyond(qc, kc):
        qs = q_pad[pl.ds(pl.multiple_of(qc * chunk, chunk), chunk), :]
        res1, total1 = tile(qs, keys_of(kc, 1), False)
        res0, total0 = tile(qs, keys_of(kc, 0), False)
        part[qc, kc] = res1 + jnp.exp2(-total1) * res0
        mass[qc, kc] = total0 + total1

    zones = []
    for n in range(n_chunks):
        zones.append(chosen(zone, [sorted(range(n_chunks), key=lambda c: (abs(c - z), c))[n] for z in range(n_chunks)]))

    def arrive(n):
        for b in range(4):
            forward(zones[n] * 4 + b)
        for b in range(4):
            take_q(zones[n] * 4 + b)

    ph("l_arrive0")
    arrive(0)
    for n in range(n_chunks):
        if n + 1 < n_chunks:
            ph(f"m{n}_arrive")
            arrive(n + 1)
        ph(f"m{n}_fwdarr")
        for b in range(4):
            forward_arrived(zones[n] * 4 + b)
        ph(f"m{n}_tiles")
        diagonal(zones[n])
        for m in range(n):
            beyond(jnp.maximum(zones[n], zones[m]), jnp.minimum(zones[n], zones[m]))
    ph("m_sum")
    for qc in range(n_chunks):
        acc = part[qc, qc]
        carry = mass[qc, qc]
        for kc in range(qc - 1, -1, -1):
            acc = acc + jnp.exp2(-carry) * part[qc, kc]
            if kc:
                carry = carry + mass[qc, kc]
        for b in range(4):
            top = acc[b * half : b * half + quarter, hd:]
            bot = acc[b * half + quarter : (b + 1) * half, hd:]
            o_send[qc * 4 + b] = jnp.concatenate([top, bot], axis=1).astype(bf)

    ph("m_give")

    def give(k, carry):
        is_self = jnp.logical_and(k == s, t == owner)

        @pl.when(is_self)
        def _():
            pltpu.make_async_copy(o_send.at[k], o_recv.at[slot, t], o_rs.at[slot, t]).start()

        @pl.when(jnp.logical_not(is_self))
        def _():
            pltpu.make_async_remote_copy(
                src_ref=o_send.at[k], dst_ref=o_recv.at[slot, t], send_sem=o_ss.at[k],
                recv_sem=o_rs.at[slot, t], device_id={"sp": k, "tp": owner}, device_id_type=MESH,
            ).start()

        return carry

    lax.fori_loop(0, n_sp, give, 0, unroll=True)

    ph("n_prev")

    @pl.when(s == 0)
    def _():
        kvw_prev[...] = jnp.zeros_like(kvw_prev)

    @pl.when(s > 0)
    def _():
        prev_copy(s - 1).wait_recv()

    ph("o_window")
    two = 2 * rows
    r_iota = lax.broadcasted_iota(jnp.int32, (two, two), 0)
    c_iota = lax.broadcasted_iota(jnp.int32, (two, two), 1)
    dist = lax.rem(r_iota, rows) + rows - c_iota
    in_window = (dist >= 0) & (dist < WINDOW) & ((c_iota >= rows) | (s > 0))
    first_rows = lax.broadcasted_iota(jnp.int32, (two, 1), 0) < rows
    for g in range(kv_heads):
        cols = slice(g * hd, (g + 1) * hd)
        v_cols = slice((kv_heads + g) * hd, (kv_heads + g + 1) * hd)
        kk = jnp.concatenate([kvw_prev[:, cols], kvw[:, cols]], axis=0)
        vv = jnp.concatenate([kvw_prev[:, v_cols], kvw[:, v_cols]], axis=0)
        base = g * GROUP * hd
        qq = jnp.concatenate(
            [qw[:, base : base + hd], qw[:, base + hd : base + 2 * hd]], axis=0
        )
        logits = jnp.where(in_window, dot_t(qq, kk) * hd**-0.5, -jnp.inf)
        sink = jnp.where(first_rows, sinks[GROUP * g], sinks[GROUP * g + 1])
        top = jnp.maximum(jnp.max(logits, axis=1, keepdims=True), sink)
        grown = jnp.exp(logits - top)
        total = jnp.sum(grown, axis=1, keepdims=True) + jnp.exp(sink - top)
        weights = (grown / total).astype(bf)
        res = dot(weights, vv)
        w_out_buf[:, base : base + 2 * hd] = jnp.concatenate([res[:rows], res[rows:]], axis=1).astype(bf)

    ph("p_sqw")
    wf = w_out_buf[...].astype(f32)
    sq_send[0] = jnp.broadcast_to(jnp.sum(wf * wf, axis=1, keepdims=True), (rows, 128))

    sq_w = to_partner(sq_send.at[0], sq_recv.at[0], sq_ss.at[0], sq_rs.at[0])
    sq_w.start()

    l_ow.wait()
    total_w[...] = dot((wf * wgain[...].reshape(1, sw)).astype(bf), vow[...])
    ph("r_takeo")

    def take_o(k, carry):
        pltpu.make_async_remote_copy(
            src_ref=o_send.at[0], dst_ref=o_recv.at[k // 2, lax.rem(k, 2)], send_sem=o_ss.at[0],
            recv_sem=o_rs.at[k // 2, lax.rem(k, 2)], device_id={"sp": s, "tp": other}, device_id_type=MESH,
        ).wait_recv()
        return carry

    lax.fori_loop(0, 2 * heads, take_o, 0, unroll=True)
    ph("s_sout")
    for j in range(heads // 2):
        for u in range(2):
            one = o_recv[2 * j, u].astype(f32)
            two_ = o_recv[2 * j + 1, u].astype(f32)
            s_out_buf[u * half : u * half + quarter, 2 * j * hd : 2 * (j + 1) * hd] = jnp.concatenate(
                [one[:, :hd], two_[:, :hd]], axis=1
            )
            s_out_buf[u * half + quarter : (u + 1) * half, 2 * j * hd : 2 * (j + 1) * hd] = jnp.concatenate(
                [one[:, hd:], two_[:, hd:]], axis=1
            )
    sf = s_out_buf[...]
    sq_send[1] = jnp.broadcast_to(jnp.sum(sf * sf, axis=1, keepdims=True), (rows, 128))
    sq_s = to_partner(sq_send.at[1], sq_recv.at[1], sq_ss.at[1], sq_rs.at[1])
    sq_s.start()
    ph("t_os")
    gained = (sf * sgain[...].reshape(1, sw)).astype(bf)
    l_os.wait()
    n_cut = c_send.shape[0]
    cut = feats // n_cut
    for n in range(n_cut):
        comb[:, n * cut : (n + 1) * cut] = dot(gained, vos[:, n * cut : (n + 1) * cut])
    sq_w.wait_recv()
    sw_cols = 2.0 * sw
    inv_w = lax.rsqrt((sq_send[0] + sq_recv[0])[:, :1] / sw_cols + EPS)
    ph("u_sqwait")
    sq_s.wait_recv()
    ph("v_csend")
    inv_s = lax.rsqrt((sq_send[1] + sq_recv[1])[:, :1] / sw_cols + EPS)
    copies = []
    theirs = pl.ds(pl.multiple_of(other * half, half), half)
    mine = pl.ds(pl.multiple_of(t * half, half), half)
    for n in range(n_cut):
        cols = slice(n * cut, (n + 1) * cut)
        comb[:, cols] = comb[:, cols] * inv_s + total_w[:, cols] * inv_w
        c_send[n] = comb[theirs, cols].astype(bf)
        copy = to_partner(c_send.at[n], c_recv.at[n], c_ss.at[n], c_rs.at[n])
        copy.start()
        copies.append(copy)

    ph("w_drain")
    x_copy.wait_send()
    b_copy.wait_send()

    def scatter_done(k, carry):
        i = k // 2
        u = lax.rem(k, 2)
        chip = 2 * i + t

        @pl.when(jnp.logical_not(jnp.logical_and(chip == s, u == t)))
        def _():
            pltpu.make_async_remote_copy(
                src_ref=kv_send.at[i, u], dst_ref=kv_all.at[s, u], send_sem=kv_ss.at[i, u],
                recv_sem=kv_rs.at[s], device_id={"sp": chip, "tp": u}, device_id_type=MESH,
            ).wait_send()

        return carry

    lax.fori_loop(0, 2 * heads, scatter_done, 0)

    def forward_sent(k, carry):
        to_partner(kv_all.at[k, t, :half], kv_all.at[k, t, :half], f_ss.at[k], f_rs.at[k]).wait_send()
        return carry

    lax.fori_loop(0, n_sp, forward_sent, 0)

    @pl.when(s < n_sp - 1)
    def _():
        prev_copy(s + 1).wait_send()

    def gave(k, carry):
        @pl.when(jnp.logical_not(jnp.logical_and(k == s, t == owner)))
        def _():
            pltpu.make_async_remote_copy(
                src_ref=o_send.at[k], dst_ref=o_recv.at[slot, t], send_sem=o_ss.at[k],
                recv_sem=o_rs.at[slot, t], device_id={"sp": k, "tp": owner}, device_id_type=MESH,
            ).wait_send()

        return carry

    lax.fori_loop(0, n_sp, gave, 0)
    sq_w.wait_send()
    sq_s.wait_send()

    ph("x_crecv")
    square = jnp.zeros((half, 1), f32)
    for n in range(n_cut):
        cols = slice(n * cut, (n + 1) * cut)
        copies[n].wait_recv()
        summed = (comb[mine, cols] + c_recv[n].astype(f32)).astype(bf).astype(f32)
        total_w[:half, cols] = summed
        square = square + jnp.sum(summed * summed, axis=1, keepdims=True)
    ph("y_out")
    inv = lax.rsqrt(square / feats + EPS)
    out[...] = (total_w[:half, :] * inv * post_gain[...].reshape(1, feats)).astype(bf)
    for copy in copies:
        copy.wait_send()
    ph(None)


SIGN = -1


def one_kernel(n_sp, *args):
    tokens, pre_gain, wqs, wks, wvs, wqw, wkw, wvw, bias, sinks, sgain, wgain, wos, wow, post_gain = args
    bf = jnp.bfloat16
    f32 = jnp.float32
    rows, feat_half = tokens.shape
    feats = 2 * feat_half
    half = rows // 2
    hd = HEAD_DIM
    heads = wqs.shape[1] // hd
    sw = wqs.shape[1]
    wide = 2 * hd
    kvw_cols = wkw.shape[1] + wvw.shape[1]
    n_chunks = n_sp // 4
    assert 2 * heads == n_sp and rows == WINDOW
    v = pltpu.VMEM
    dma = pltpu.SemaphoreType.DMA
    anywhere = pl.BlockSpec(memory_space=pl.ANY)
    vmem = pl.BlockSpec(memory_space=pltpu.VMEM)
    n_cut = 4
    split = lambda w: v((2, w.shape[0] // 2, w.shape[1]), bf)
    scratch = [
        v(pre_gain.shape, f32), pltpu.SMEM(bias.shape, f32), pltpu.SMEM(sinks.shape, f32),
        v(sgain.shape, f32), v(wgain.shape, f32), v(post_gain.shape, f32),
        v((2, rows, feat_half), bf), v((2, heads, 128), f32), v((2, rows, feat_half), bf),
        split(wqs), split(wks), split(wvs), split(wqw), split(wkw), split(wvw), v(wos.shape, bf), v(wow.shape, bf),
        v((3, rows, sw), f32),
        v((heads, 2, half + half // 2, wide), bf), v((n_sp, 2, half + half // 2, wide), bf),
        v((n_sp * half, wide), bf),
        v((n_chunks, n_chunks, 4 * half, wide), f32), v((n_chunks, n_chunks, 4 * half, wide), f32),
        v((rows, sw), bf), v((rows, kvw_cols), bf), v((rows, kvw_cols), bf), v((rows, sw), bf),
        v((n_sp, half // 2, wide), bf), v((heads, 2, half // 2, wide), bf), v((rows, sw), f32),
        v((2, rows, 128), f32), v((2, rows, 128), f32), v((rows, feats), f32), v((rows, feats), f32),
        v((n_cut, half, feats // n_cut), bf), v((n_cut, half, feats // n_cut), bf),
        dma((14,)), dma((6,)), dma, dma, dma, dma, dma, dma((heads, 2)), dma((n_sp,)),
        dma((n_sp,)), dma((n_sp,)), dma, dma, dma((n_sp,)), dma((heads, 2)), dma((2,)), dma((2,)),
        dma((n_cut,)), dma((n_cut,)),
    ]
    return pl.pallas_call(
        functools.partial(kernel, n_sp),
        out_shape=pltpu.VMEM((half, feats), bf),
        in_specs=[anywhere] * len(args),
        out_specs=vmem,
        scratch_shapes=scratch,
        compiler_params=pltpu.CompilerParams(
            collective_id=0, has_side_effects=True, vmem_limit_bytes=60 * 1024 * 1024
        ),
        name="layer",
    )(*[pltpu.with_memory_space_constraint(a, pltpu.HBM) for a in args])


def passed_along(value, axis, steps):
    count = lax.axis_size(axis)
    initial, last = (max(0, -steps), min(count, count - steps))
    return lax.ppermute(value, axis, [(source, source + steps) for source in range(initial, last)])


def rounded(values):
    return lax.optimization_barrier(values.astype(jnp.bfloat16)).astype(jnp.float32)


def norm_rows(values, gain):
    stats = jnp.mean(values * values, axis=-1, keepdims=True)
    return values * lax.rsqrt(stats + EPS) * gain


def stick_block(queries, key_pair, head_bias, key_mask, carried):
    result, logsum = carried
    head_count = queries.shape[1]
    key_rows = key_pair[0].reshape(key_pair.shape[1], head_count, HEAD_DIM)
    values = key_pair[1].reshape(key_pair.shape[1], head_count, HEAD_DIM)
    scores = jnp.einsum(
        "thd,shd->hts", queries, key_rows, preferred_element_type=jnp.float32
    ) * HEAD_DIM ** (-0.5)
    scores = scores + head_bias[:, None, None]
    usable = key_mask[None]
    log_keep = jnp.where(usable, jax.nn.log_sigmoid(-scores), 0.0)
    suffix = lax.cumsum(log_keep, axis=2, reverse=True) - log_keep
    stick_weights = jnp.where(
        usable, jnp.exp(jax.nn.log_sigmoid(scores) + suffix + logsum[:, :, None]), 0.0
    )
    stick_weights = stick_weights.astype(jnp.bfloat16)
    result = result + jnp.einsum(
        "hts,shd->htd", stick_weights, values, preferred_element_type=jnp.float32
    )
    logsum = logsum + jnp.sum(log_keep, axis=2)
    return (result, logsum)


def by_collectives(
    tokens,
    pre_gain,
    w_query_stick,
    w_key_stick,
    w_value_stick,
    w_query_window,
    w_key_window,
    w_value_window,
    stick_bias,
    sinks,
    stick_gain,
    window_gain,
    w_out_stick,
    w_out_window,
    post_gain,
):
    gathered = lax.all_gather(tokens, "tp", axis=1, tiled=True)
    normed = norm_rows(gathered.astype(jnp.float32), pre_gain).astype(jnp.bfloat16)

    def project(weight):
        return jnp.dot(normed, weight, preferred_element_type=jnp.float32).astype(jnp.bfloat16)

    tok_rows = normed.shape[0]
    dev_index = lax.axis_index("sp")
    dev_count = lax.axis_size("sp")
    query_stick = project(w_query_stick)
    stick_heads = query_stick.shape[1] // HEAD_DIM
    queries = query_stick.reshape(tok_rows, stick_heads, HEAD_DIM)
    own_pair = jnp.stack([project(w_key_stick), project(w_value_stick)])
    pair_width = own_pair.shape[2]
    positions = jnp.arange(tok_rows, dtype=jnp.int32)
    initial = (
        jnp.zeros((stick_heads, tok_rows, HEAD_DIM), jnp.float32),
        jnp.zeros((stick_heads, tok_rows), jnp.float32),
    )
    collected = own_pair[None]
    for section_index in range(dev_count.bit_length() - 1):
        arrived = passed_along(collected, "sp", 2**section_index)
        collected = jnp.concatenate([arrived, collected], axis=0)
    per_group = min(dev_count, 8)
    group_count = dev_count // per_group
    grouped = collected.reshape(group_count, per_group, 2, tok_rows, pair_width)
    grouped = grouped.transpose(0, 2, 1, 3, 4).reshape(
        group_count, 2, per_group * tok_rows, pair_width
    )
    first_source = dev_index - (dev_count - 1)
    group_starts = (first_source + jnp.arange(group_count, dtype=jnp.int32) * per_group) * tok_rows
    query_pos = dev_index * tok_rows + positions
    span_offs = jnp.arange(per_group * tok_rows, dtype=jnp.int32)

    def visit_group(carried, inputs):
        key_pair, start_pos = inputs
        key_pos = start_pos + span_offs
        key_mask = (key_pos[None, :] >= 0) & (key_pos[None, :] < query_pos[:, None])
        return (stick_block(queries, key_pair, stick_bias, key_mask, carried), None)

    (stick_sum, _), _ = lax.scan(visit_group, initial, (grouped, group_starts), reverse=True)
    stick_out = (
        stick_sum.transpose(1, 0, 2).reshape(tok_rows, stick_heads * HEAD_DIM).astype(jnp.bfloat16)
    )
    query_window = project(w_query_window)
    window_pair = jnp.stack([project(w_key_window), project(w_value_window)])
    kv_heads = window_pair.shape[2] // HEAD_DIM
    previous = passed_along(window_pair, "sp", 1)
    extended = jnp.concatenate([previous, window_pair], axis=1)
    block_count = tok_rows // WINDOW
    extended = extended.reshape(2, block_count + 1, WINDOW, kv_heads, HEAD_DIM)
    banded = jnp.concatenate([extended[:, :-1], extended[:, 1:]], axis=2)
    q_blocks = query_window.reshape(block_count, WINDOW, kv_heads, GROUP, HEAD_DIM)
    logits = jnp.einsum(
        "nqhgd,nchd->nhgqc", q_blocks, banded[0], preferred_element_type=jnp.float32
    ) * HEAD_DIM ** (-0.5)
    query_offs = jnp.arange(WINDOW, dtype=jnp.int32)[:, None]
    key_offs = jnp.arange(2 * WINDOW, dtype=jnp.int32)[None, :]
    distance = query_offs + WINDOW - key_offs
    key_pos = (
        dev_index * tok_rows
        + jnp.arange(block_count, dtype=jnp.int32)[:, None] * WINDOW
        - WINDOW
        + key_offs
    )
    usable = ((distance >= 0) & (distance < WINDOW))[None] & (key_pos >= 0)[:, None, :]
    logits = jnp.where(usable[:, None, None], logits, -jnp.inf)
    sink_logit = sinks.reshape(kv_heads, GROUP)[None, :, :, None, None]
    row_top = jnp.maximum(jnp.max(logits, axis=-1, keepdims=True), sink_logit)
    weights_exp = jnp.exp(logits - row_top)
    normalizer = jnp.sum(weights_exp, axis=-1, keepdims=True) + jnp.exp(sink_logit - row_top)
    window_weights = (weights_exp / normalizer).astype(jnp.bfloat16)
    window_sum = jnp.einsum(
        "nhgqc,nchd->nqhgd", window_weights, banded[1], preferred_element_type=jnp.float32
    )
    window_out = window_sum.reshape(tok_rows, query_window.shape[1]).astype(jnp.bfloat16)
    stick_float = stick_out.astype(jnp.float32)
    window_float = window_out.astype(jnp.float32)
    squares = lax.psum(
        (jnp.sum(stick_float * stick_float, axis=1), jnp.sum(window_float * window_float, axis=1)),
        "tp",
    )
    stick_normed = (
        stick_float * lax.rsqrt(squares[0][:, None] / (stick_gain.shape[0] * lax.axis_size("tp")) + EPS) * stick_gain
    ).astype(jnp.bfloat16)
    window_normed = (
        window_float * lax.rsqrt(squares[1][:, None] / (window_gain.shape[0] * lax.axis_size("tp")) + EPS) * window_gain
    ).astype(jnp.bfloat16)
    total = jnp.dot(stick_normed, w_out_stick, preferred_element_type=jnp.float32)
    combined = lax.psum_scatter(
        (total + jnp.dot(window_normed, w_out_window, preferred_element_type=jnp.float32)).astype(
            jnp.bfloat16
        ),
        "tp",
        scatter_dimension=0,
        tiled=True,
    ).astype(jnp.float32)
    combined = rounded(combined)
    return norm_rows(combined, post_gain).astype(jnp.bfloat16)


def solution(mesh):
    in_specs = (
        P("sp", "tp"),
        P(),
        P(None, "tp"),
        P(None, "tp"),
        P(None, "tp"),
        P(None, "tp"),
        P(None, "tp"),
        P(None, "tp"),
        P("tp"),
        P("tp"),
        P("tp"),
        P("tp"),
        P("tp", None),
        P("tp", None),
        P(),
    )
    n_sp, n_tp = mesh.shape["sp"], mesh.shape["tp"]

    def shards(*args):
        heads = args[2].shape[1] // HEAD_DIM
        if n_tp == 2 and n_tp * heads == n_sp and args[0].shape[0] == WINDOW and n_sp % 4 == 0:
            return one_kernel(n_sp, *args)
        return by_collectives(*args)

    return jax.shard_map(
        shards,
        mesh=mesh,
        in_specs=in_specs,
        out_specs=P(("sp", "tp"), None),
        check_vma=False,
    )
```

```python
import functools

import jax
import jax.numpy as jnp
from jax import lax
from jax.experimental import pallas as pl
from jax.experimental.pallas import tpu as pltpu
from jax.sharding import PartitionSpec as P

HEAD_DIM = 64
GROUP = 2
WINDOW = 128
EPS = 1e-06
LOG2E = 1.4426950408889634
MESH = pl.DeviceIdType.MESH


class Phases:
    def __init__(self):
        self.scope = None

    def __call__(self, name):
        if self.scope is not None:
            self.scope.__exit__(None, None, None)
            self.scope = None
        if name:
            self.scope = jax.named_scope(name)
            self.scope.__enter__()


def dot(a, b):
    return jnp.dot(a, b, preferred_element_type=jnp.float32)


def dot_t(a, b):
    return lax.dot_general(a, b, (((1,), (1,)), ((), ())), preferred_element_type=jnp.float32)


def chosen(at, table):
    value = jnp.int32(table[0])
    for n in range(1, len(table)):
        if table[n] != table[0]:
            value = jnp.where(at == n, jnp.int32(table[n]), value)
    return value


def zone_order(z, count):
    return sorted(range(count), key=lambda c: (2 * c // count != 2 * z // count, abs(c - z)))


def send_order(z, count):
    return sorted(range(count), key=lambda c: (abs(c - z), 2 * c // count != 2 * z // count))


def kernel(
    n_sp,
    tokens, pre_gain_in, wqs, wks, wvs, wqw, wkw, wvw, bias_in, sinks_in, sgain_in, wgain_in, wos, wow,
    post_gain_in, out,
    pre_gain, bias, sinks, sgain, wgain, post_gain, x, bias_buf, xg, vqs, vks, vvs, vqw, vkw, vvw, vos, vow,
    proj, kv_send, kv_all, q_pad, part, mass,
    qw, kvw, kvw_prev, w_out_buf, o_send, o_recv, s_out_buf,
    sq_send, sq_recv, total_w, comb, c_send, c_recv, wc_send, wc_recv,
    w_sem, small_sem, tok_sem, x_ss, x_rs, b_ss, b_rs, kv_ss, kv_rs, f_ss, f_rs,
    p_ss, p_rs, o_ss, o_rs, sq_ss, sq_rs, c_ss, c_rs, wc_ss, wc_rs, hello, all_in,
):
    bf = jnp.bfloat16
    f32 = jnp.float32
    s = lax.axis_index("sp")
    t = lax.axis_index("tp")
    other = 1 - t
    rows, feat_half = tokens.shape
    feats = 2 * feat_half
    half = rows // 2
    quarter = half // 2
    hd = HEAD_DIM
    heads = wqs.shape[1] // hd
    kv_heads = wkw.shape[1] // hd
    sw = wqs.shape[1]
    n_chunks = n_sp // 4
    ph = Phases()
    ph("a_entry")

    tok_load = pltpu.make_async_copy(tokens, x.at[0], tok_sem)
    tok_load.start()
    smalls = [
        pltpu.make_async_copy(src, dst, small_sem.at[n])
        for n, (src, dst) in enumerate(
            [(bias_in, bias), (pre_gain_in, pre_gain), (sinks_in, sinks), (sgain_in, sgain),
             (wgain_in, wgain), (post_gain_in, post_gain)]
        )
    ]
    for load in smalls:
        load.start()

    barrier = pltpu.get_barrier_semaphore()
    partner = {"sp": s, "tp": other}

    @pl.when(t == 0)
    def _():
        pl.semaphore_signal(barrier, inc=1, device_id=partner, device_id_type=MESH)

    def greet(k, carry):
        pl.semaphore_signal(
            barrier, inc=1, device_id={"sp": lax.rem(s + k, n_sp), "tp": 0}, device_id_type=MESH
        )
        return carry

    lax.fori_loop(1, n_sp, greet, 0, unroll=True)

    own_rows = pl.ds(pl.multiple_of(t * feat_half, feat_half), feat_half)
    other_rows = pl.ds(pl.multiple_of(other * feat_half, feat_half), feat_half)
    loads = {}
    for n, (name, src, dst) in enumerate(
        [("ks", wks, vks), ("vs", wvs, vvs), ("qs", wqs, vqs), ("kw", wkw, vkw), ("vw", wvw, vvw), ("qw", wqw, vqw)]
    ):
        loads[name] = [
            pltpu.make_async_copy(src.at[own_rows], dst.at[0], w_sem.at[2 * n]),
            pltpu.make_async_copy(src.at[other_rows], dst.at[1], w_sem.at[2 * n + 1]),
        ]
    l_ow = pltpu.make_async_copy(wow, vow, w_sem.at[12])
    l_os = pltpu.make_async_copy(wos, vos, w_sem.at[13])

    for part_of in range(2):
        for name in ("ks", "vs", "qs"):
            loads[name][part_of].start()
    ph("b_hello")

    @pl.when(t == 1)
    def _():
        pl.semaphore_wait(barrier, 1)
        pl.semaphore_signal(hello, inc=1, device_id=partner, device_id_type=MESH)

    @pl.when(t == 0)
    def _():
        pl.semaphore_wait(hello, 1)

    def to_partner(src, dst, ss, rs):
        return pltpu.make_async_remote_copy(
            src_ref=src, dst_ref=dst, send_sem=ss, recv_sem=rs,
            device_id={"sp": s, "tp": other}, device_id_type=MESH,
        )

    ph("b_tokwait")
    tok_load.wait()
    x_copy = to_partner(x.at[0], x.at[1], x_ss, x_rs)
    x_copy.start()
    for load in smalls:
        load.wait()

    row_id = lax.broadcasted_iota(jnp.int32, (heads, 128), 0)
    bias_rows = jnp.zeros((heads, 128), f32)
    for i in range(heads):
        bias_rows = jnp.where(row_id == i, bias[i] * LOG2E, bias_rows)
    bias_buf[t] = bias_rows

    ph("c_gain")
    gain = pre_gain[...].reshape(1, feats)
    gains = [
        jnp.where(t == 0, gain[:, :feat_half], gain[:, feat_half:]),
        jnp.where(t == 0, gain[:, feat_half:], gain[:, :feat_half]),
    ]

    def scaled(n):
        value = x[n].astype(f32)
        xg[n] = (value * gains[n]).astype(bf)
        return jnp.sum(value * value, axis=1, keepdims=True)

    squares = scaled(0)

    b_copy = to_partner(bias_buf.at[t], bias_buf.at[t], b_ss, b_rs)
    b_copy.start()

    ph("e_own")
    for n, (name, w) in enumerate([("ks", vks), ("vs", vvs), ("qs", vqs)]):
        loads[name][0].wait()
        proj[n] = dot(xg[0], w[0])
    for name in ("kw", "vw", "qw"):
        for load in loads[name]:
            load.start()
    ph("f_xwait")
    x_copy.wait_recv()
    ph("g_kvq")
    for name in ("ks", "vs", "qs"):
        loads[name][1].wait()
    inv = lax.rsqrt((squares + scaled(1)) * (1.0 / feats) + EPS)
    keys = (proj[0] + dot(xg[1], vks[1])) * inv
    values = (proj[1] + dot(xg[1], vvs[1])) * inv
    for i in range(heads):
        cols = slice(i * hd, (i + 1) * hd)
        packed = jnp.concatenate([keys[:, cols], values[:, cols]], axis=1).astype(bf)
        kv_send[i, :, :half] = packed.reshape(2, half, 2 * hd)
    queries = (proj[2] + dot(xg[1], vqs[1])) * (inv * (LOG2E * hd**-0.5))
    for i in range(heads):
        cols = slice(i * hd, (i + 1) * hd)
        for u in range(2):
            top = queries[u * half : u * half + quarter, cols]
            low = queries[u * half + quarter : (u + 1) * half, cols]
            kv_send[i, u, half:] = jnp.concatenate([top, low], axis=1).astype(bf)

    ph("h_barrier")

    @pl.when(t == 0)
    def _():
        pl.semaphore_wait(barrier, 2 * (n_sp - 1))
        pl.semaphore_signal(all_in, inc=1, device_id=partner, device_id_type=MESH)

    @pl.when(t == 1)
    def _():
        pl.semaphore_wait(all_in, 1)

    ph("i_scatter")
    zone = s // 4
    owner = lax.rem(s, 2)
    slot = s // 2

    def dest_order(n):
        by_zone = []
        for z in range(n_chunks):
            order = [2 * c + y for c in send_order(z, n_chunks) for y in range(2)]
            by_zone.append(order[n])
        return chosen(zone, by_zone)

    for n in range(heads):
        i = dest_order(n)
        chip = 2 * i + t
        for u in range(2):
            is_self = jnp.logical_and(chip == s, u == t)

            @pl.when(is_self)
            def _():
                pltpu.make_async_copy(kv_send.at[i, u], kv_all.at[s, u], kv_rs.at[s]).start()

            @pl.when(jnp.logical_not(is_self))
            def _():
                pltpu.make_async_remote_copy(
                    src_ref=kv_send.at[i, u], dst_ref=kv_all.at[s, u], send_sem=kv_ss.at[i, u],
                    recv_sem=kv_rs.at[s], device_id={"sp": chip, "tp": u}, device_id_type=MESH,
                ).start()

    ph("j_wproj")
    l_ow.start()
    l_os.start()
    for load in loads["kw"] + loads["vw"]:
        load.wait()
    kvw[:, : kv_heads * hd] = ((dot(xg[0], vkw[0]) + dot(xg[1], vkw[1])) * inv).astype(bf)
    kvw[:, kv_heads * hd :] = ((dot(xg[0], vvw[0]) + dot(xg[1], vvw[1])) * inv).astype(bf)
    prev_copy = lambda to: pltpu.make_async_remote_copy(
        src_ref=kvw, dst_ref=kvw_prev, send_sem=p_ss, recv_sem=p_rs,
        device_id={"sp": to, "tp": t}, device_id_type=MESH,
    )

    @pl.when(s < n_sp - 1)
    def _():
        prev_copy(s + 1).start()

    for load in loads["qw"]:
        load.wait()
    qw[...] = ((dot(xg[0], vqw[0]) + dot(xg[1], vqw[1])) * inv).astype(bf)

    ph("k_misc")

    def forward(src):
        pltpu.make_async_remote_copy(
            src_ref=kv_send.at[0, 0], dst_ref=kv_all.at[src, t], send_sem=kv_ss.at[0, 0],
            recv_sem=kv_rs.at[src], device_id={"sp": s, "tp": other}, device_id_type=MESH,
        ).wait_recv()
        to_partner(kv_all.at[src, t, :half], kv_all.at[src, t, :half], f_ss.at[src], f_rs.at[src]).start()

    def forward_arrived(k):
        to_partner(kv_all.at[k, other, :half], kv_all.at[k, other, :half], f_ss.at[k], f_rs.at[k]).wait_recv()

    def take_q(k):
        slab = kv_all[k, t, half:].astype(f32)
        zero = jnp.zeros((quarter, hd), f32)
        both = jnp.concatenate(
            [
                jnp.concatenate([slab[:, :hd], zero], axis=1),
                jnp.concatenate([slab[:, hd:], zero], axis=1),
            ],
            axis=0,
        )
        q_pad[pl.ds(pl.multiple_of(k * half, half), half), :] = both.astype(bf)

    b_copy.wait_recv()
    head_bias = bias_buf[owner, pl.ds(slot, 1), :][:, :1]

    kt = 2 * rows
    later = (
        lax.broadcasted_iota(jnp.int32, (kt, kt), 0) > lax.broadcasted_iota(jnp.int32, (kt, kt), 1)
    ).astype(bf)
    row = lax.broadcasted_iota(jnp.int32, (rows, kt), 0)
    lane = lax.broadcasted_iota(jnp.int32, (rows, kt), 1)
    before = lane < (row // half) * rows + t * half + lax.rem(row, half)

    def weigh(tiles):
        drops, holds = [], []
        for qs, kv, masked in tiles:
            z = dot_t(qs, kv) + head_bias
            pos = jnp.maximum(z, 0.0)
            drop = pos + jnp.log2(1.0 + jnp.exp2(z - pos - pos))
            hold = z - drop
            if masked:
                drop_top = jnp.where(before, drop[:rows], 0.0)
                hold_top = jnp.where(before, hold[:rows], -jnp.inf)
                if drop.shape[0] == rows:
                    drop, hold = drop_top, hold_top
                else:
                    drop = jnp.concatenate([drop_top, drop[rows:]], axis=0)
                    hold = jnp.concatenate([hold_top, hold[rows:]], axis=0)
            drops.append(drop)
            holds.append(hold)
        suffixes = [dot(drop.astype(bf), later) for drop in drops]
        results = []
        for (_, kv, _), drop, hold, suffix in zip(tiles, drops, holds, suffixes):
            total = jnp.broadcast_to(suffix[:, :1] + drop[:, :1], (drop.shape[0], 2 * hd))
            results.append((dot(jnp.exp2(hold - suffix).astype(bf), kv), total))
        return results

    def keys_of(g):
        return kv_all[pl.ds(2 * g, 2), :, :half].reshape(kt, 2 * hd)

    def queries_of(g, count):
        return q_pad[pl.ds(pl.multiple_of(g * rows, rows), count * rows), :]

    def take_zone(c, others):
        places = [(2 * c + 1, 2 * c + 1, 1, True), (2 * c, 2 * c, 2, True)]
        for e in others:
            qc, kc = jnp.maximum(c, e), jnp.minimum(c, e)
            places += [(2 * qc, 2 * kc, 2, False), (2 * qc, 2 * kc + 1, 2, False)]
        step = 4
        for n in range(0, len(places), step):
            some = places[n : n + step]
            results = weigh([(queries_of(q, count), keys_of(g), masked) for q, g, count, masked in some])
            for (q, g, count, _), (res, total) in zip(some, results):
                part[g, pl.ds(q, count)] = res.reshape(count, rows, 2 * hd)
                mass[g, pl.ds(q, count)] = total.reshape(count, rows, 2 * hd)

    def finish(g):
        def add(j, carry):
            acc, passed = carry
            k = g - j
            return acc + jnp.exp2(-passed) * part[k, g], passed + mass[k, g]

        acc, _ = lax.fori_loop(1, g + 1, add, (part[g, g], mass[g, g]))
        for b in range(2):
            top = acc[b * half : b * half + quarter, hd:]
            bot = acc[b * half + quarter : (b + 1) * half, hd:]
            o_send[2 * g + b] = jnp.concatenate([top, bot], axis=1).astype(bf)
        for b in range(2):
            k = 2 * g + b
            is_self = jnp.logical_and(k == s, t == owner)

            @pl.when(is_self)
            def _():
                pltpu.make_async_copy(o_send.at[k], o_recv.at[slot, t], o_rs.at[slot, t]).start()

            @pl.when(jnp.logical_not(is_self))
            def _():
                pltpu.make_async_remote_copy(
                    src_ref=o_send.at[k], dst_ref=o_recv.at[slot, t], send_sem=o_ss.at[k],
                    recv_sem=o_rs.at[slot, t], device_id={"sp": k, "tp": owner}, device_id_type=MESH,
                ).start()

    def finish_range(lo, hi):
        def step(g, carry):
            finish(g)
            return carry

        lax.fori_loop(lo, hi, step, 0)

    takes = [zone_order(z, n_chunks) for z in range(n_chunks)]
    units = []
    for z in range(n_chunks):
        mine_units = [[2 * c, 2 * c + 1] for c in takes[z]]
        units.append(mine_units)
    n_units = len(units[0])
    ends = []
    for z in range(n_chunks):
        seen, done, spans = set(), 0, []
        for unit in units[z]:
            seen |= set(unit)
            upto = done
            while upto in seen:
                upto += 1
            spans.append((done, upto))
            done = upto
        ends.append(spans)
    group = [[chosen(zone, [units[z][n][m] for z in range(n_chunks)]) for m in range(len(units[0][n]))] for n in range(n_units)]

    def arrive(n):
        for g in group[n]:
            for b in range(2):
                forward(2 * g + b)
        for g in group[n]:
            for b in range(2):
                take_q(2 * g + b)

    def arrived(n):
        for g in group[n]:
            for b in range(2):
                forward_arrived(2 * g + b)

    ph("l_arrive0")
    arrive(0)
    for n in range(n_units):
        if n + 1 < n_units:
            ph(f"m{n}_arrive")
            arrive(n + 1)
        ph(f"m{n}_fwdarr")
        arrived(n)
        ph(f"m{n}_tiles")
        take_zone(group[n][0] // 2, [group[m][0] // 2 for m in range(n)])
        ph(f"m{n}_finish")
        finish_range(chosen(zone, [ends[z][n][0] for z in range(n_chunks)]), chosen(zone, [ends[z][n][1] for z in range(n_chunks)]))

    ph("n_prev")

    @pl.when(s == 0)
    def _():
        kvw_prev[...] = jnp.zeros_like(kvw_prev)

    @pl.when(s > 0)
    def _():
        prev_copy(s - 1).wait_recv()

    ph("o_window")
    two = 2 * rows
    r_iota = lax.broadcasted_iota(jnp.int32, (two, two), 0)
    c_iota = lax.broadcasted_iota(jnp.int32, (two, two), 1)
    dist = lax.rem(r_iota, rows) + rows - c_iota
    in_window = (dist >= 0) & (dist < WINDOW) & ((c_iota >= rows) | (s > 0))
    first_rows = lax.broadcasted_iota(jnp.int32, (two, 1), 0) < rows
    for g in range(kv_heads):
        cols = slice(g * hd, (g + 1) * hd)
        v_cols = slice((kv_heads + g) * hd, (kv_heads + g + 1) * hd)
        kk = jnp.concatenate([kvw_prev[:, cols], kvw[:, cols]], axis=0)
        vv = jnp.concatenate([kvw_prev[:, v_cols], kvw[:, v_cols]], axis=0)
        base = g * GROUP * hd
        qq = jnp.concatenate(
            [qw[:, base : base + hd], qw[:, base + hd : base + 2 * hd]], axis=0
        )
        logits = jnp.where(in_window, dot_t(qq, kk) * hd**-0.5, -jnp.inf)
        sink = jnp.where(first_rows, sinks[GROUP * g], sinks[GROUP * g + 1])
        top = jnp.maximum(jnp.max(logits, axis=1, keepdims=True), sink)
        grown = jnp.exp(logits - top)
        total = jnp.sum(grown, axis=1, keepdims=True) + jnp.exp(sink - top)
        weights = (grown / total).astype(bf)
        res = dot(weights, vv)
        w_out_buf[:, base : base + 2 * hd] = jnp.concatenate([res[:rows], res[rows:]], axis=1).astype(bf)

    ph("p_sqw")
    theirs = pl.ds(pl.multiple_of(other * half, half), half)
    mine = pl.ds(pl.multiple_of(t * half, half), half)
    n_cut = c_send.shape[0]
    cut = feats // n_cut

    def squares_to_partner(n, squared):
        sq_send[n] = jnp.broadcast_to(jnp.sum(squared, axis=1, keepdims=True), (rows, 128))
        copy = to_partner(sq_send.at[n, theirs], sq_recv.at[n], sq_ss.at[n], sq_rs.at[n])
        copy.start()
        return copy

    def halves_to_partner(left, weights, total, send, recv, ss, rs):
        copies = []
        for n in range(n_cut):
            cols = slice(n * cut, (n + 1) * cut)
            total[:, cols] = dot(left, weights[:, cols])
            send[n] = total[theirs, cols].astype(bf)
            copy = to_partner(send.at[n], recv.at[n], ss.at[n], rs.at[n])
            copy.start()
            copies.append(copy)
        return copies

    wf = w_out_buf[...].astype(f32)
    sq_w = squares_to_partner(0, wf * wf)
    l_ow.wait()
    w_copies = halves_to_partner((wf * wgain[...].reshape(1, sw)).astype(bf), vow, total_w, wc_send, wc_recv, wc_ss, wc_rs)
    ph("r_takeo")

    def take_o(k, carry):
        pltpu.make_async_remote_copy(
            src_ref=o_send.at[0], dst_ref=o_recv.at[k // 2, lax.rem(k, 2)], send_sem=o_ss.at[0],
            recv_sem=o_rs.at[k // 2, lax.rem(k, 2)], device_id={"sp": s, "tp": other}, device_id_type=MESH,
        ).wait_recv()
        return carry

    lax.fori_loop(0, 2 * heads, take_o, 0, unroll=True)
    ph("s_sout")
    for j in range(heads // 2):
        for u in range(2):
            one = o_recv[2 * j, u].astype(f32)
            two_ = o_recv[2 * j + 1, u].astype(f32)
            s_out_buf[u * half : u * half + quarter, 2 * j * hd : 2 * (j + 1) * hd] = jnp.concatenate(
                [one[:, :hd], two_[:, :hd]], axis=1
            )
            s_out_buf[u * half + quarter : (u + 1) * half, 2 * j * hd : 2 * (j + 1) * hd] = jnp.concatenate(
                [one[:, hd:], two_[:, hd:]], axis=1
            )
    sf = s_out_buf[...]
    sq_s = squares_to_partner(1, sf * sf)
    ph("t_os")
    l_os.wait()
    copies = halves_to_partner((sf * sgain[...].reshape(1, sw)).astype(bf), vos, comb, c_send, c_recv, c_ss, c_rs)
    ph("u_wsum")
    sw_cols = 2.0 * sw
    sq_w.wait_recv()
    inv_w = lax.rsqrt((sq_send[0, mine] + sq_recv[0])[:, :1] / sw_cols + EPS)
    for n in range(n_cut):
        cols = slice(n * cut, (n + 1) * cut)
        w_copies[n].wait_recv()
        total_w[:half, cols] = (total_w[mine, cols] + wc_recv[n].astype(f32)) * inv_w

    ph("w_drain")
    x_copy.wait_send()
    b_copy.wait_send()

    def scatter_done(k, carry):
        i = k // 2
        u = lax.rem(k, 2)
        chip = 2 * i + t

        @pl.when(jnp.logical_not(jnp.logical_and(chip == s, u == t)))
        def _():
            pltpu.make_async_remote_copy(
                src_ref=kv_send.at[i, u], dst_ref=kv_all.at[s, u], send_sem=kv_ss.at[i, u],
                recv_sem=kv_rs.at[s], device_id={"sp": chip, "tp": u}, device_id_type=MESH,
            ).wait_send()

        return carry

    lax.fori_loop(0, 2 * heads, scatter_done, 0)

    def forward_sent(k, carry):
        to_partner(kv_all.at[k, t, :half], kv_all.at[k, t, :half], f_ss.at[k], f_rs.at[k]).wait_send()
        return carry

    lax.fori_loop(0, n_sp, forward_sent, 0)

    @pl.when(s < n_sp - 1)
    def _():
        prev_copy(s + 1).wait_send()

    def gave(k, carry):
        @pl.when(jnp.logical_not(jnp.logical_and(k == s, t == owner)))
        def _():
            pltpu.make_async_remote_copy(
                src_ref=o_send.at[k], dst_ref=o_recv.at[slot, t], send_sem=o_ss.at[k],
                recv_sem=o_rs.at[slot, t], device_id={"sp": k, "tp": owner}, device_id_type=MESH,
            ).wait_send()

        return carry

    lax.fori_loop(0, n_sp, gave, 0)
    sq_w.wait_send()
    sq_s.wait_send()

    ph("x_sqrecv")
    sq_s.wait_recv()
    inv_s = lax.rsqrt((sq_send[1, mine] + sq_recv[1])[:, :1] / sw_cols + EPS)
    ph("x_crecv")
    square = jnp.zeros((half, 1), f32)
    for n in range(n_cut):
        cols = slice(n * cut, (n + 1) * cut)
        copies[n].wait_recv()
        summed = (comb[mine, cols] + c_recv[n].astype(f32)) * inv_s + total_w[:half, cols]
        summed = summed.astype(bf).astype(f32)
        total_w[:half, cols] = summed
        square = square + jnp.sum(summed * summed, axis=1, keepdims=True)
    ph("y_out")
    inv = lax.rsqrt(square / feats + EPS)
    out[...] = (total_w[:half, :] * inv * post_gain[...].reshape(1, feats)).astype(bf)
    for copy in copies + w_copies:
        copy.wait_send()
    ph(None)


def one_kernel(n_sp, *args):
    tokens, pre_gain, wqs, wks, wvs, wqw, wkw, wvw, bias, sinks, sgain, wgain, wos, wow, post_gain = args
    bf = jnp.bfloat16
    f32 = jnp.float32
    rows, feat_half = tokens.shape
    feats = 2 * feat_half
    half = rows // 2
    hd = HEAD_DIM
    heads = wqs.shape[1] // hd
    sw = wqs.shape[1]
    wide = 2 * hd
    kvw_cols = wkw.shape[1] + wvw.shape[1]
    n_chunks = n_sp // 4
    assert 2 * heads == n_sp and rows == WINDOW
    v = pltpu.VMEM
    dma = pltpu.SemaphoreType.DMA
    anywhere = pl.BlockSpec(memory_space=pl.ANY)
    vmem = pl.BlockSpec(memory_space=pltpu.VMEM)
    n_cut = 4
    split = lambda w: v((2, w.shape[0] // 2, w.shape[1]), bf)
    scratch = [
        v(pre_gain.shape, f32), pltpu.SMEM(bias.shape, f32), pltpu.SMEM(sinks.shape, f32),
        v(sgain.shape, f32), v(wgain.shape, f32), v(post_gain.shape, f32),
        v((2, rows, feat_half), bf), v((2, heads, 128), f32), v((2, rows, feat_half), bf),
        split(wqs), split(wks), split(wvs), split(wqw), split(wkw), split(wvw), v(wos.shape, bf), v(wow.shape, bf),
        v((3, rows, sw), f32),
        v((heads, 2, half + half // 2, wide), bf), v((n_sp, 2, half + half // 2, wide), bf),
        v((n_sp * half, wide), bf),
        v((2 * n_chunks, 2 * n_chunks, rows, wide), f32), v((2 * n_chunks, 2 * n_chunks, rows, wide), f32),
        v((rows, sw), bf), v((rows, kvw_cols), bf), v((rows, kvw_cols), bf), v((rows, sw), bf),
        v((n_sp, half // 2, wide), bf), v((heads, 2, half // 2, wide), bf), v((rows, sw), f32),
        v((2, rows, 128), f32), v((2, half, 128), f32), v((rows, feats), f32), v((rows, feats), f32),
        v((n_cut, half, feats // n_cut), bf), v((n_cut, half, feats // n_cut), bf),
        v((n_cut, half, feats // n_cut), bf), v((n_cut, half, feats // n_cut), bf),
        dma((14,)), dma((6,)), dma, dma, dma, dma, dma, dma((heads, 2)), dma((n_sp,)),
        dma((n_sp,)), dma((n_sp,)), dma, dma, dma((n_sp,)), dma((heads, 2)), dma((2,)), dma((2,)),
        dma((n_cut,)), dma((n_cut,)), dma((n_cut,)), dma((n_cut,)), pltpu.SemaphoreType.REGULAR, pltpu.SemaphoreType.REGULAR,
    ]
    return pl.pallas_call(
        functools.partial(kernel, n_sp),
        out_shape=pltpu.VMEM((half, feats), bf),
        in_specs=[anywhere] * len(args),
        out_specs=vmem,
        scratch_shapes=scratch,
        compiler_params=pltpu.CompilerParams(
            collective_id=0, has_side_effects=True, vmem_limit_bytes=60 * 1024 * 1024
        ),
        name="layer",
    )(*[pltpu.with_memory_space_constraint(a, pltpu.HBM) for a in args])


def passed_along(value, axis, steps):
    count = lax.axis_size(axis)
    initial, last = (max(0, -steps), min(count, count - steps))
    return lax.ppermute(value, axis, [(source, source + steps) for source in range(initial, last)])


def rounded(values):
    return lax.optimization_barrier(values.astype(jnp.bfloat16)).astype(jnp.float32)


def norm_rows(values, gain):
    stats = jnp.mean(values * values, axis=-1, keepdims=True)
    return values * lax.rsqrt(stats + EPS) * gain


def stick_block(queries, key_pair, head_bias, key_mask, carried):
    result, logsum = carried
    head_count = queries.shape[1]
    key_rows = key_pair[0].reshape(key_pair.shape[1], head_count, HEAD_DIM)
    values = key_pair[1].reshape(key_pair.shape[1], head_count, HEAD_DIM)
    scores = jnp.einsum(
        "thd,shd->hts", queries, key_rows, preferred_element_type=jnp.float32
    ) * HEAD_DIM ** (-0.5)
    scores = scores + head_bias[:, None, None]
    usable = key_mask[None]
    log_keep = jnp.where(usable, jax.nn.log_sigmoid(-scores), 0.0)
    suffix = lax.cumsum(log_keep, axis=2, reverse=True) - log_keep
    stick_weights = jnp.where(
        usable, jnp.exp(jax.nn.log_sigmoid(scores) + suffix + logsum[:, :, None]), 0.0
    )
    stick_weights = stick_weights.astype(jnp.bfloat16)
    result = result + jnp.einsum(
        "hts,shd->htd", stick_weights, values, preferred_element_type=jnp.float32
    )
    logsum = logsum + jnp.sum(log_keep, axis=2)
    return (result, logsum)


def by_collectives(
    tokens,
    pre_gain,
    w_query_stick,
    w_key_stick,
    w_value_stick,
    w_query_window,
    w_key_window,
    w_value_window,
    stick_bias,
    sinks,
    stick_gain,
    window_gain,
    w_out_stick,
    w_out_window,
    post_gain,
):
    gathered = lax.all_gather(tokens, "tp", axis=1, tiled=True)
    normed = norm_rows(gathered.astype(jnp.float32), pre_gain).astype(jnp.bfloat16)

    def project(weight):
        return jnp.dot(normed, weight, preferred_element_type=jnp.float32).astype(jnp.bfloat16)

    tok_rows = normed.shape[0]
    dev_index = lax.axis_index("sp")
    dev_count = lax.axis_size("sp")
    query_stick = project(w_query_stick)
    stick_heads = query_stick.shape[1] // HEAD_DIM
    queries = query_stick.reshape(tok_rows, stick_heads, HEAD_DIM)
    own_pair = jnp.stack([project(w_key_stick), project(w_value_stick)])
    pair_width = own_pair.shape[2]
    positions = jnp.arange(tok_rows, dtype=jnp.int32)
    initial = (
        jnp.zeros((stick_heads, tok_rows, HEAD_DIM), jnp.float32),
        jnp.zeros((stick_heads, tok_rows), jnp.float32),
    )
    collected = own_pair[None]
    for section_index in range(dev_count.bit_length() - 1):
        arrived = passed_along(collected, "sp", 2**section_index)
        collected = jnp.concatenate([arrived, collected], axis=0)
    per_group = min(dev_count, 8)
    group_count = dev_count // per_group
    grouped = collected.reshape(group_count, per_group, 2, tok_rows, pair_width)
    grouped = grouped.transpose(0, 2, 1, 3, 4).reshape(
        group_count, 2, per_group * tok_rows, pair_width
    )
    first_source = dev_index - (dev_count - 1)
    group_starts = (first_source + jnp.arange(group_count, dtype=jnp.int32) * per_group) * tok_rows
    query_pos = dev_index * tok_rows + positions
    span_offs = jnp.arange(per_group * tok_rows, dtype=jnp.int32)

    def visit_group(carried, inputs):
        key_pair, start_pos = inputs
        key_pos = start_pos + span_offs
        key_mask = (key_pos[None, :] >= 0) & (key_pos[None, :] < query_pos[:, None])
        return (stick_block(queries, key_pair, stick_bias, key_mask, carried), None)

    (stick_sum, _), _ = lax.scan(visit_group, initial, (grouped, group_starts), reverse=True)
    stick_out = (
        stick_sum.transpose(1, 0, 2).reshape(tok_rows, stick_heads * HEAD_DIM).astype(jnp.bfloat16)
    )
    query_window = project(w_query_window)
    window_pair = jnp.stack([project(w_key_window), project(w_value_window)])
    kv_heads = window_pair.shape[2] // HEAD_DIM
    previous = passed_along(window_pair, "sp", 1)
    extended = jnp.concatenate([previous, window_pair], axis=1)
    block_count = tok_rows // WINDOW
    extended = extended.reshape(2, block_count + 1, WINDOW, kv_heads, HEAD_DIM)
    banded = jnp.concatenate([extended[:, :-1], extended[:, 1:]], axis=2)
    q_blocks = query_window.reshape(block_count, WINDOW, kv_heads, GROUP, HEAD_DIM)
    logits = jnp.einsum(
        "nqhgd,nchd->nhgqc", q_blocks, banded[0], preferred_element_type=jnp.float32
    ) * HEAD_DIM ** (-0.5)
    query_offs = jnp.arange(WINDOW, dtype=jnp.int32)[:, None]
    key_offs = jnp.arange(2 * WINDOW, dtype=jnp.int32)[None, :]
    distance = query_offs + WINDOW - key_offs
    key_pos = (
        dev_index * tok_rows
        + jnp.arange(block_count, dtype=jnp.int32)[:, None] * WINDOW
        - WINDOW
        + key_offs
    )
    usable = ((distance >= 0) & (distance < WINDOW))[None] & (key_pos >= 0)[:, None, :]
    logits = jnp.where(usable[:, None, None], logits, -jnp.inf)
    sink_logit = sinks.reshape(kv_heads, GROUP)[None, :, :, None, None]
    row_top = jnp.maximum(jnp.max(logits, axis=-1, keepdims=True), sink_logit)
    weights_exp = jnp.exp(logits - row_top)
    normalizer = jnp.sum(weights_exp, axis=-1, keepdims=True) + jnp.exp(sink_logit - row_top)
    window_weights = (weights_exp / normalizer).astype(jnp.bfloat16)
    window_sum = jnp.einsum(
        "nhgqc,nchd->nqhgd", window_weights, banded[1], preferred_element_type=jnp.float32
    )
    window_out = window_sum.reshape(tok_rows, query_window.shape[1]).astype(jnp.bfloat16)
    stick_float = stick_out.astype(jnp.float32)
    window_float = window_out.astype(jnp.float32)
    squares = lax.psum(
        (jnp.sum(stick_float * stick_float, axis=1), jnp.sum(window_float * window_float, axis=1)),
        "tp",
    )
    stick_normed = (
        stick_float * lax.rsqrt(squares[0][:, None] / (stick_gain.shape[0] * lax.axis_size("tp")) + EPS) * stick_gain
    ).astype(jnp.bfloat16)
    window_normed = (
        window_float * lax.rsqrt(squares[1][:, None] / (window_gain.shape[0] * lax.axis_size("tp")) + EPS) * window_gain
    ).astype(jnp.bfloat16)
    total = jnp.dot(stick_normed, w_out_stick, preferred_element_type=jnp.float32)
    combined = lax.psum_scatter(
        (total + jnp.dot(window_normed, w_out_window, preferred_element_type=jnp.float32)).astype(
            jnp.bfloat16
        ),
        "tp",
        scatter_dimension=0,
        tiled=True,
    ).astype(jnp.float32)
    combined = rounded(combined)
    return norm_rows(combined, post_gain).astype(jnp.bfloat16)


def solution(mesh):
    in_specs = (
        P("sp", "tp"),
        P(),
        P(None, "tp"),
        P(None, "tp"),
        P(None, "tp"),
        P(None, "tp"),
        P(None, "tp"),
        P(None, "tp"),
        P("tp"),
        P("tp"),
        P("tp"),
        P("tp"),
        P("tp", None),
        P("tp", None),
        P(),
    )
    n_sp, n_tp = mesh.shape["sp"], mesh.shape["tp"]

    def shards(*args):
        heads = args[2].shape[1] // HEAD_DIM
        if n_tp == 2 and n_tp * heads == n_sp and args[0].shape[0] == WINDOW and n_sp % 4 == 0:
            return one_kernel(n_sp, *args)
        return by_collectives(*args)

    return jax.shard_map(
        shards,
        mesh=mesh,
        in_specs=in_specs,
        out_specs=P(("sp", "tp"), None),
        check_vma=False,
    )
```

```python
import functools

import jax
import jax.numpy as jnp
from jax import lax
from jax.experimental import pallas as pl
from jax.experimental.pallas import tpu as pltpu
from jax.sharding import PartitionSpec as P

HEAD_DIM = 64
GROUP = 2
WINDOW = 128
EPS = 1e-06
LOG2E = 1.4426950408889634
MESH = pl.DeviceIdType.MESH


class Phases:
    def __init__(self):
        self.scope = None

    def __call__(self, name):
        if self.scope is not None:
            self.scope.__exit__(None, None, None)
            self.scope = None
        if name:
            self.scope = jax.named_scope(name)
            self.scope.__enter__()


def dot(a, b):
    return jnp.dot(a, b, preferred_element_type=jnp.float32)


def dot_t(a, b):
    return lax.dot_general(a, b, (((1,), (1,)), ((), ())), preferred_element_type=jnp.float32)


def chosen(at, table):
    value = jnp.int32(table[0])
    for n in range(1, len(table)):
        if table[n] != table[0]:
            value = jnp.where(at == n, jnp.int32(table[n]), value)
    return value


def zone_order(z, count):
    return sorted(range(count), key=lambda c: (2 * c // count != 2 * z // count, abs(c - z)))


def send_order(z, count):
    near = [c for c in zone_order(z, count) if 2 * c // count == 2 * z // count]
    far = [c for c in reversed(range(count)) if c not in near]
    if z >= count // 2:
        far.reverse()
    inside = [(c, y) for c in near for y in range(2)]
    across = [(c, (y + n) % 2) for y in range(2) for n, c in enumerate(far)]
    return inside + across if IN_FIRST else across + inside


IN_FIRST = False
AHEAD = 4


def kernel(
    n_sp,
    tokens, pre_gain_in, wqs, wks, wvs, wqw, wkw, wvw, bias_in, sinks_in, sgain_in, wgain_in, wos, wow,
    post_gain_in, out,
    pre_gain, bias, sinks, sgain, wgain, post_gain, x, bias_buf, xg, vqs, vks, vvs, vqw, vkw, vvw, vos, vow,
    proj, kv_send, kv_all, q_pad, acc, mass,
    qw, kvw, kvw_prev, w_out_buf, o_send, o_recv, s_out_buf,
    sq_send, sq_recv, total_w, comb, c_send, c_recv, wc_send, wc_recv,
    w_sem, small_sem, tok_sem, x_ss, x_rs, b_ss, b_rs, kv_ss, kv_rs, f_ss, f_rs,
    p_ss, p_rs, o_ss, o_rs, sq_ss, sq_rs, c_ss, c_rs, wc_ss, wc_rs, hello, all_in,
):
    bf = jnp.bfloat16
    f32 = jnp.float32
    s = lax.axis_index("sp")
    t = lax.axis_index("tp")
    other = 1 - t
    rows, feat_half = tokens.shape
    feats = 2 * feat_half
    half = rows // 2
    quarter = half // 2
    hd = HEAD_DIM
    heads = wqs.shape[1] // hd
    kv_heads = wkw.shape[1] // hd
    sw = wqs.shape[1]
    n_chunks = n_sp // 4
    ph = Phases()
    ph("a_entry")

    tok_load = pltpu.make_async_copy(tokens, x.at[0], tok_sem)
    tok_load.start()
    smalls = [
        pltpu.make_async_copy(src, dst, small_sem.at[n])
        for n, (src, dst) in enumerate(
            [(bias_in, bias), (pre_gain_in, pre_gain), (sinks_in, sinks), (sgain_in, sgain),
             (wgain_in, wgain), (post_gain_in, post_gain)]
        )
    ]
    for load in smalls:
        load.start()

    barrier = pltpu.get_barrier_semaphore()
    partner = {"sp": s, "tp": other}

    @pl.when(t == 0)
    def _():
        pl.semaphore_signal(barrier, inc=1, device_id=partner, device_id_type=MESH)

    def greet(k, carry):
        pl.semaphore_signal(
            barrier, inc=1, device_id={"sp": lax.rem(s + k, n_sp), "tp": 0}, device_id_type=MESH
        )
        return carry

    lax.fori_loop(1, n_sp, greet, 0, unroll=True)

    own_rows = pl.ds(pl.multiple_of(t * feat_half, feat_half), feat_half)
    other_rows = pl.ds(pl.multiple_of(other * feat_half, feat_half), feat_half)
    loads = {}
    for n, (name, src, dst) in enumerate(
        [("ks", wks, vks), ("vs", wvs, vvs), ("qs", wqs, vqs), ("kw", wkw, vkw), ("vw", wvw, vvw), ("qw", wqw, vqw)]
    ):
        loads[name] = [
            pltpu.make_async_copy(src.at[own_rows], dst.at[0], w_sem.at[2 * n]),
            pltpu.make_async_copy(src.at[other_rows], dst.at[1], w_sem.at[2 * n + 1]),
        ]
    l_ow = pltpu.make_async_copy(wow, vow, w_sem.at[12])
    l_os = pltpu.make_async_copy(wos, vos, w_sem.at[13])

    for part_of in range(2):
        for name in ("ks", "vs", "qs"):
            loads[name][part_of].start()
    ph("b_hello")

    @pl.when(t == 1)
    def _():
        pl.semaphore_wait(barrier, 1)
        pl.semaphore_signal(hello, inc=1, device_id=partner, device_id_type=MESH)

    @pl.when(t == 0)
    def _():
        pl.semaphore_wait(hello, 1)

    def to_partner(src, dst, ss, rs):
        return pltpu.make_async_remote_copy(
            src_ref=src, dst_ref=dst, send_sem=ss, recv_sem=rs,
            device_id={"sp": s, "tp": other}, device_id_type=MESH,
        )

    ph("b_tokwait")
    tok_load.wait()
    x_copy = to_partner(x.at[0], x.at[1], x_ss, x_rs)
    x_copy.start()
    for load in smalls:
        load.wait()

    row_id = lax.broadcasted_iota(jnp.int32, (heads, 128), 0)
    bias_rows = jnp.zeros((heads, 128), f32)
    for i in range(heads):
        bias_rows = jnp.where(row_id == i, bias[i] * LOG2E, bias_rows)
    bias_buf[t] = bias_rows

    ph("c_gain")
    gain = pre_gain[...].reshape(1, feats)
    gains = [
        jnp.where(t == 0, gain[:, :feat_half], gain[:, feat_half:]),
        jnp.where(t == 0, gain[:, feat_half:], gain[:, :feat_half]),
    ]

    def scaled(n):
        value = x[n].astype(f32)
        xg[n] = (value * gains[n]).astype(bf)
        return jnp.sum(value * value, axis=1, keepdims=True)

    squares = scaled(0)

    b_copy = to_partner(bias_buf.at[t], bias_buf.at[t], b_ss, b_rs)
    b_copy.start()

    ph("e_own")
    for n, (name, w) in enumerate([("ks", vks), ("vs", vvs), ("qs", vqs)]):
        loads[name][0].wait()
        proj[n] = dot(xg[0], w[0])
    for name in ("kw", "vw", "qw"):
        for load in loads[name]:
            load.start()
    ph("f_xwait")
    x_copy.wait_recv()
    ph("g_kvq")
    for name in ("ks", "vs", "qs"):
        loads[name][1].wait()
    inv = lax.rsqrt((squares + scaled(1)) * (1.0 / feats) + EPS)
    keys = (proj[0] + dot(xg[1], vks[1])) * inv
    values = (proj[1] + dot(xg[1], vvs[1])) * inv
    for i in range(heads):
        cols = slice(i * hd, (i + 1) * hd)
        packed = jnp.concatenate([keys[:, cols], values[:, cols]], axis=1).astype(bf)
        kv_send[i, :, :half] = packed.reshape(2, half, 2 * hd)
    queries = (proj[2] + dot(xg[1], vqs[1])) * (inv * (LOG2E * hd**-0.5))
    for i in range(heads):
        cols = slice(i * hd, (i + 1) * hd)
        for u in range(2):
            top = queries[u * half : u * half + quarter, cols]
            low = queries[u * half + quarter : (u + 1) * half, cols]
            kv_send[i, u, half:] = jnp.concatenate([top, low], axis=1).astype(bf)

    ph("h_barrier")

    @pl.when(t == 0)
    def _():
        pl.semaphore_wait(barrier, 2 * (n_sp - 1))
        pl.semaphore_signal(all_in, inc=1, device_id=partner, device_id_type=MESH)

    @pl.when(t == 1)
    def _():
        pl.semaphore_wait(all_in, 1)

    ph("i_scatter")
    zone = s // 4
    owner = lax.rem(s, 2)
    slot = s // 2

    def dest_order(n):
        by_zone = []
        for z in range(n_chunks):
            order = [2 * c + y for c, y in send_order(z, n_chunks)]
            by_zone.append(order[n])
        return chosen(zone, by_zone)

    for n in range(heads):
        i = dest_order(n)
        chip = 2 * i + t
        for u in range(2):
            is_self = jnp.logical_and(chip == s, u == t)

            @pl.when(is_self)
            def _():
                pltpu.make_async_copy(kv_send.at[i, u], kv_all.at[s, u], kv_rs.at[s]).start()

            @pl.when(jnp.logical_not(is_self))
            def _():
                pltpu.make_async_remote_copy(
                    src_ref=kv_send.at[i, u], dst_ref=kv_all.at[s, u], send_sem=kv_ss.at[i, u],
                    recv_sem=kv_rs.at[s], device_id={"sp": chip, "tp": u}, device_id_type=MESH,
                ).start()

    ph("j_wproj")
    l_ow.start()
    l_os.start()
    for load in loads["kw"] + loads["vw"]:
        load.wait()
    kvw[:, : kv_heads * hd] = ((dot(xg[0], vkw[0]) + dot(xg[1], vkw[1])) * inv).astype(bf)
    kvw[:, kv_heads * hd :] = ((dot(xg[0], vvw[0]) + dot(xg[1], vvw[1])) * inv).astype(bf)
    prev_copy = lambda to: pltpu.make_async_remote_copy(
        src_ref=kvw, dst_ref=kvw_prev, send_sem=p_ss, recv_sem=p_rs,
        device_id={"sp": to, "tp": t}, device_id_type=MESH,
    )

    @pl.when(s < n_sp - 1)
    def _():
        prev_copy(s + 1).start()

    for load in loads["qw"]:
        load.wait()
    qw[...] = ((dot(xg[0], vqw[0]) + dot(xg[1], vqw[1])) * inv).astype(bf)

    ph("k_misc")

    def forward(src):
        pltpu.make_async_remote_copy(
            src_ref=kv_send.at[0, 0], dst_ref=kv_all.at[src, t], send_sem=kv_ss.at[0, 0],
            recv_sem=kv_rs.at[src], device_id={"sp": s, "tp": other}, device_id_type=MESH,
        ).wait_recv()
        to_partner(kv_all.at[src, t, :half], kv_all.at[src, t, :half], f_ss.at[src], f_rs.at[src]).start()

    def forward_arrived(k):
        to_partner(kv_all.at[k, other, :half], kv_all.at[k, other, :half], f_ss.at[k], f_rs.at[k]).wait_recv()

    def take_q(k):
        slab = kv_all[k, t, half:].astype(f32)
        zero = jnp.zeros((quarter, hd), f32)
        both = jnp.concatenate(
            [
                jnp.concatenate([slab[:, :hd], zero], axis=1),
                jnp.concatenate([slab[:, hd:], zero], axis=1),
            ],
            axis=0,
        )
        q_pad[pl.ds(pl.multiple_of(k * half, half), half), :] = both.astype(bf)

    b_copy.wait_recv()
    head_bias = bias_buf[owner, pl.ds(slot, 1), :][:, :1]

    kt = 2 * rows
    later = (
        lax.broadcasted_iota(jnp.int32, (kt, kt), 0) > lax.broadcasted_iota(jnp.int32, (kt, kt), 1)
    ).astype(bf)
    row = lax.broadcasted_iota(jnp.int32, (rows, kt), 0)
    lane = lax.broadcasted_iota(jnp.int32, (rows, kt), 1)
    before = lane < (row // half) * rows + t * half + lax.rem(row, half)

    def weigh(tiles):
        drops, holds = [], []
        for qs, kv, masked in tiles:
            z = dot_t(qs, kv) + head_bias
            pos = jnp.maximum(z, 0.0)
            drop = pos + jnp.log2(1.0 + jnp.exp2(z - pos - pos))
            hold = z - drop
            if masked:
                drop_top = jnp.where(before, drop[:rows], 0.0)
                hold_top = jnp.where(before, hold[:rows], -jnp.inf)
                if drop.shape[0] == rows:
                    drop, hold = drop_top, hold_top
                else:
                    drop = jnp.concatenate([drop_top, drop[rows:]], axis=0)
                    hold = jnp.concatenate([hold_top, hold[rows:]], axis=0)
            drops.append(drop)
            holds.append(hold)
        suffixes = [dot(drop.astype(bf), later) for drop in drops]
        results = []
        for (_, kv, _), drop, hold, suffix in zip(tiles, drops, holds, suffixes):
            total = jnp.broadcast_to(suffix[:, :1] + drop[:, :1], (drop.shape[0], 2 * hd))
            results.append((dot(jnp.exp2(hold - suffix).astype(bf), kv), total))
        return results

    def keys_of(g):
        return kv_all[pl.ds(2 * g, 2), :, :half].reshape(kt, 2 * hd)

    def queries_of(g, count):
        return q_pad[pl.ds(pl.multiple_of(g * rows, rows), count * rows), :]

    def put(q, g, count, result, first):
        res, total = (value.reshape(count, rows, 2 * hd) for value in result)
        at = pl.ds(q, count)
        if first:
            acc[at] = res
            mass[at] = total
        else:
            passed = mass[at]
            acc[at] = acc[at] + jnp.exp2(-passed) * res
            mass[at] = passed + total

    def give(c):
        for g in range(2):
            value = acc[2 * c + g]
            for b in range(2):
                top = value[b * half : b * half + quarter, hd:]
                bot = value[b * half + quarter : (b + 1) * half, hd:]
                o_send[4 * c + 2 * g + b] = jnp.concatenate([top, bot], axis=1).astype(bf)
        for b in range(4):
            k = 4 * c + b
            is_self = jnp.logical_and(k == s, t == owner)

            @pl.when(is_self)
            def _():
                pltpu.make_async_copy(o_send.at[k], o_recv.at[slot, t], o_rs.at[slot, t]).start()

            @pl.when(jnp.logical_not(is_self))
            def _():
                pltpu.make_async_remote_copy(
                    src_ref=o_send.at[k], dst_ref=o_recv.at[slot, t], send_sem=o_ss.at[k],
                    recv_sem=o_rs.at[slot, t], device_id={"sp": k, "tp": owner}, device_id_type=MESH,
                ).start()

    takes = [zone_order(z, n_chunks) for z in range(n_chunks)]
    batches = []
    for n in range(n_chunks):
        partners = [sorted(takes[z][:n], reverse=True) for z in range(n_chunks)]
        steps = [[None] + list(range(min(n, 1)))] + [list(range(m, min(m + 2, n))) for m in range(1, n, 2)]
        batches.append((partners, steps))
    seen = [set() for _ in range(n_chunks)]
    given = [set() for _ in range(n_chunks)]

    def arrive(n):
        c = chosen(zone, [takes[z][n] for z in range(n_chunks)])
        for b in range(4):
            forward(4 * c + b)
        for b in range(4):
            take_q(4 * c + b)

    def take(n):
        c = chosen(zone, [takes[z][n] for z in range(n_chunks)])
        for b in range(4):
            forward_arrived(4 * c + b)
        partners, steps = batches[n]
        for step in steps:
            places = []
            for m in step:
                if m is None:
                    places += [(2 * c + 1, 2 * c + 1, 1, True), (2 * c, 2 * c, 2, True)]
                else:
                    e = chosen(zone, [partners[z][m] for z in range(n_chunks)])
                    qc, kc = jnp.maximum(c, e), jnp.minimum(c, e)
                    places += [(2 * qc, 2 * kc + 1, 2, False), (2 * qc, 2 * kc, 2, False)]
            results = weigh([(queries_of(q, count), keys_of(g), masked) for q, g, count, masked in places])
            if step[0] is None:
                (res1, total1), (res0, total0) = results[:2]
                at = pl.ds(2 * c, 2)
                acc[at] = jnp.concatenate(
                    [res0[:rows], res1 + jnp.exp2(-total1) * res0[rows:]], axis=0
                ).reshape(2, rows, 2 * hd)
                mass[at] = jnp.concatenate([total0[:rows], total1 + total0[rows:]], axis=0).reshape(2, rows, 2 * hd)
            for (q, g, count, masked), result in zip(places, results):
                if not masked:
                    put(q, g, count, result, False)
            ready = []
            for z in range(n_chunks):
                for m in step:
                    a, b = takes[z][n], takes[z][n] if m is None else partners[z][m]
                    seen[z].add((max(a, b), min(a, b)))
                ready.append([
                    q for q in range(n_chunks)
                    if q not in given[z] and all((q, k) in seen[z] for k in range(q + 1))
                ])
                given[z] |= set(ready[z])
            for j in range(max(len(r) for r in ready)):
                lasts = chosen(zone, [r[j] if j < len(r) else 0 for r in ready])
                if all(j < len(r) for r in ready):
                    give(lasts)
                else:
                    @pl.when(chosen(zone, [int(j < len(r)) for r in ready]) == 1)
                    def _():
                        give(lasts)

    ph("l_arrive0")
    arrive(0)
    for n in range(n_chunks):
        if n + 1 < n_chunks:
            ph(f"m{n}_arrive")
            arrive(n + 1)
        ph(f"m{n}_take")
        take(n)

    ph("n_prev")

    @pl.when(s == 0)
    def _():
        kvw_prev[...] = jnp.zeros_like(kvw_prev)

    @pl.when(s > 0)
    def _():
        prev_copy(s - 1).wait_recv()

    ph("o_window")
    two = 2 * rows
    r_iota = lax.broadcasted_iota(jnp.int32, (two, two), 0)
    c_iota = lax.broadcasted_iota(jnp.int32, (two, two), 1)
    dist = lax.rem(r_iota, rows) + rows - c_iota
    in_window = (dist >= 0) & (dist < WINDOW) & ((c_iota >= rows) | (s > 0))
    first_rows = lax.broadcasted_iota(jnp.int32, (two, 1), 0) < rows
    for g in range(kv_heads):
        cols = slice(g * hd, (g + 1) * hd)
        v_cols = slice((kv_heads + g) * hd, (kv_heads + g + 1) * hd)
        kk = jnp.concatenate([kvw_prev[:, cols], kvw[:, cols]], axis=0)
        vv = jnp.concatenate([kvw_prev[:, v_cols], kvw[:, v_cols]], axis=0)
        base = g * GROUP * hd
        qq = jnp.concatenate(
            [qw[:, base : base + hd], qw[:, base + hd : base + 2 * hd]], axis=0
        )
        logits = jnp.where(in_window, dot_t(qq, kk) * hd**-0.5, -jnp.inf)
        sink = jnp.where(first_rows, sinks[GROUP * g], sinks[GROUP * g + 1])
        top = jnp.maximum(jnp.max(logits, axis=1, keepdims=True), sink)
        grown = jnp.exp(logits - top)
        total = jnp.sum(grown, axis=1, keepdims=True) + jnp.exp(sink - top)
        weights = (grown / total).astype(bf)
        res = dot(weights, vv)
        w_out_buf[:, base : base + 2 * hd] = jnp.concatenate([res[:rows], res[rows:]], axis=1).astype(bf)

    ph("p_sqw")
    theirs = pl.ds(pl.multiple_of(other * half, half), half)
    mine = pl.ds(pl.multiple_of(t * half, half), half)
    n_cut = c_send.shape[0]
    cut = feats // n_cut

    def squares_to_partner(n, squared):
        sq_send[n] = jnp.broadcast_to(jnp.sum(squared, axis=1, keepdims=True), (rows, 128))
        copy = to_partner(sq_send.at[n, theirs], sq_recv.at[n], sq_ss.at[n], sq_rs.at[n])
        copy.start()
        return copy

    def halves_to_partner(left, weights, total, send, recv, ss, rs):
        copies = []

        def give_half(n):
            send[n] = total[theirs, n * cut : (n + 1) * cut].astype(bf)
            copy = to_partner(send.at[n], recv.at[n], ss.at[n], rs.at[n])
            copy.start()
            copies.append(copy)

        for n in range(n_cut):
            cols = slice(n * cut, (n + 1) * cut)
            total[:, cols] = dot(left, weights[:, cols])
            if n >= AHEAD:
                give_half(n - AHEAD)
        for n in range(n_cut - AHEAD, n_cut):
            give_half(n)
        return copies

    wf = w_out_buf[...].astype(f32)
    sq_w = squares_to_partner(0, wf * wf)
    l_ow.wait()
    w_copies = halves_to_partner((wf * wgain[...].reshape(1, sw)).astype(bf), vow, total_w, wc_send, wc_recv, wc_ss, wc_rs)
    ph("r_takeo")

    def take_o(k, carry):
        pltpu.make_async_remote_copy(
            src_ref=o_send.at[0], dst_ref=o_recv.at[k // 2, lax.rem(k, 2)], send_sem=o_ss.at[0],
            recv_sem=o_rs.at[k // 2, lax.rem(k, 2)], device_id={"sp": s, "tp": other}, device_id_type=MESH,
        ).wait_recv()
        return carry

    lax.fori_loop(0, 2 * heads, take_o, 0, unroll=True)
    ph("s_sout")
    for j in range(heads // 2):
        for u in range(2):
            one = o_recv[2 * j, u].astype(f32)
            two_ = o_recv[2 * j + 1, u].astype(f32)
            s_out_buf[u * half : u * half + quarter, 2 * j * hd : 2 * (j + 1) * hd] = jnp.concatenate(
                [one[:, :hd], two_[:, :hd]], axis=1
            )
            s_out_buf[u * half + quarter : (u + 1) * half, 2 * j * hd : 2 * (j + 1) * hd] = jnp.concatenate(
                [one[:, hd:], two_[:, hd:]], axis=1
            )
    sf = s_out_buf[...]
    sq_s = squares_to_partner(1, sf * sf)
    ph("t_os")
    l_os.wait()
    copies = halves_to_partner((sf * sgain[...].reshape(1, sw)).astype(bf), vos, comb, c_send, c_recv, c_ss, c_rs)
    ph("u_wsum")
    sw_cols = 2.0 * sw
    sq_w.wait_recv()
    inv_w = lax.rsqrt((sq_send[0, mine] + sq_recv[0])[:, :1] / sw_cols + EPS)
    for n in range(n_cut):
        cols = slice(n * cut, (n + 1) * cut)
        w_copies[n].wait_recv()
        total_w[:half, cols] = (total_w[mine, cols] + wc_recv[n].astype(f32)) * inv_w

    ph("w_drain")
    x_copy.wait_send()
    b_copy.wait_send()

    def scatter_done(k, carry):
        i = k // 2
        u = lax.rem(k, 2)
        chip = 2 * i + t

        @pl.when(jnp.logical_not(jnp.logical_and(chip == s, u == t)))
        def _():
            pltpu.make_async_remote_copy(
                src_ref=kv_send.at[i, u], dst_ref=kv_all.at[s, u], send_sem=kv_ss.at[i, u],
                recv_sem=kv_rs.at[s], device_id={"sp": chip, "tp": u}, device_id_type=MESH,
            ).wait_send()

        return carry

    lax.fori_loop(0, 2 * heads, scatter_done, 0, unroll=True)

    def forward_sent(k, carry):
        to_partner(kv_all.at[k, t, :half], kv_all.at[k, t, :half], f_ss.at[k], f_rs.at[k]).wait_send()
        return carry

    lax.fori_loop(0, n_sp, forward_sent, 0, unroll=True)

    @pl.when(s < n_sp - 1)
    def _():
        prev_copy(s + 1).wait_send()

    def gave(k, carry):
        @pl.when(jnp.logical_not(jnp.logical_and(k == s, t == owner)))
        def _():
            pltpu.make_async_remote_copy(
                src_ref=o_send.at[k], dst_ref=o_recv.at[slot, t], send_sem=o_ss.at[k],
                recv_sem=o_rs.at[slot, t], device_id={"sp": k, "tp": owner}, device_id_type=MESH,
            ).wait_send()

        return carry

    lax.fori_loop(0, n_sp, gave, 0, unroll=True)
    sq_w.wait_send()
    sq_s.wait_send()

    ph("x_sqrecv")
    sq_s.wait_recv()
    inv_s = lax.rsqrt((sq_send[1, mine] + sq_recv[1])[:, :1] / sw_cols + EPS)
    ph("x_crecv")
    square = jnp.zeros((half, 1), f32)
    for n in range(n_cut):
        cols = slice(n * cut, (n + 1) * cut)
        copies[n].wait_recv()
        summed = (comb[mine, cols] + c_recv[n].astype(f32)) * inv_s + total_w[:half, cols]
        summed = summed.astype(bf).astype(f32)
        total_w[:half, cols] = summed
        square = square + jnp.sum(summed * summed, axis=1, keepdims=True)
    ph("y_out")
    inv = lax.rsqrt(square / feats + EPS)
    out[...] = (total_w[:half, :] * inv * post_gain[...].reshape(1, feats)).astype(bf)
    for copy in copies + w_copies:
        copy.wait_send()
    ph(None)


def one_kernel(n_sp, *args):
    tokens, pre_gain, wqs, wks, wvs, wqw, wkw, wvw, bias, sinks, sgain, wgain, wos, wow, post_gain = args
    bf = jnp.bfloat16
    f32 = jnp.float32
    rows, feat_half = tokens.shape
    feats = 2 * feat_half
    half = rows // 2
    hd = HEAD_DIM
    heads = wqs.shape[1] // hd
    sw = wqs.shape[1]
    wide = 2 * hd
    kvw_cols = wkw.shape[1] + wvw.shape[1]
    n_chunks = n_sp // 4
    assert 2 * heads == n_sp and rows == WINDOW
    v = pltpu.VMEM
    dma = pltpu.SemaphoreType.DMA
    anywhere = pl.BlockSpec(memory_space=pl.ANY)
    vmem = pl.BlockSpec(memory_space=pltpu.VMEM)
    n_cut = 4
    split = lambda w: v((2, w.shape[0] // 2, w.shape[1]), bf)
    scratch = [
        v(pre_gain.shape, f32), pltpu.SMEM(bias.shape, f32), pltpu.SMEM(sinks.shape, f32),
        v(sgain.shape, f32), v(wgain.shape, f32), v(post_gain.shape, f32),
        v((2, rows, feat_half), bf), v((2, heads, 128), f32), v((2, rows, feat_half), bf),
        split(wqs), split(wks), split(wvs), split(wqw), split(wkw), split(wvw), v(wos.shape, bf), v(wow.shape, bf),
        v((3, rows, sw), f32),
        v((heads, 2, half + half // 2, wide), bf), v((n_sp, 2, half + half // 2, wide), bf),
        v((n_sp * half, wide), bf),
        v((2 * n_chunks, rows, wide), f32), v((2 * n_chunks, rows, wide), f32),
        v((rows, sw), bf), v((rows, kvw_cols), bf), v((rows, kvw_cols), bf), v((rows, sw), bf),
        v((n_sp, half // 2, wide), bf), v((heads, 2, half // 2, wide), bf), v((rows, sw), f32),
        v((2, rows, 128), f32), v((2, half, 128), f32), v((rows, feats), f32), v((rows, feats), f32),
        v((n_cut, half, feats // n_cut), bf), v((n_cut, half, feats // n_cut), bf),
        v((n_cut, half, feats // n_cut), bf), v((n_cut, half, feats // n_cut), bf),
        dma((14,)), dma((6,)), dma, dma, dma, dma, dma, dma((heads, 2)), dma((n_sp,)),
        dma((n_sp,)), dma((n_sp,)), dma, dma, dma((n_sp,)), dma((heads, 2)), dma((2,)), dma((2,)),
        dma((n_cut,)), dma((n_cut,)), dma((n_cut,)), dma((n_cut,)), pltpu.SemaphoreType.REGULAR, pltpu.SemaphoreType.REGULAR,
    ]
    return pl.pallas_call(
        functools.partial(kernel, n_sp),
        out_shape=pltpu.VMEM((half, feats), bf),
        in_specs=[anywhere] * len(args),
        out_specs=vmem,
        scratch_shapes=scratch,
        compiler_params=pltpu.CompilerParams(
            collective_id=0, has_side_effects=True, vmem_limit_bytes=60 * 1024 * 1024
        ),
        name="layer",
    )(*[pltpu.with_memory_space_constraint(a, pltpu.HBM) for a in args])


def passed_along(value, axis, steps):
    count = lax.axis_size(axis)
    initial, last = (max(0, -steps), min(count, count - steps))
    return lax.ppermute(value, axis, [(source, source + steps) for source in range(initial, last)])


def rounded(values):
    return lax.optimization_barrier(values.astype(jnp.bfloat16)).astype(jnp.float32)


def norm_rows(values, gain):
    stats = jnp.mean(values * values, axis=-1, keepdims=True)
    return values * lax.rsqrt(stats + EPS) * gain


def stick_block(queries, key_pair, head_bias, key_mask, carried):
    result, logsum = carried
    head_count = queries.shape[1]
    key_rows = key_pair[0].reshape(key_pair.shape[1], head_count, HEAD_DIM)
    values = key_pair[1].reshape(key_pair.shape[1], head_count, HEAD_DIM)
    scores = jnp.einsum(
        "thd,shd->hts", queries, key_rows, preferred_element_type=jnp.float32
    ) * HEAD_DIM ** (-0.5)
    scores = scores + head_bias[:, None, None]
    usable = key_mask[None]
    log_keep = jnp.where(usable, jax.nn.log_sigmoid(-scores), 0.0)
    suffix = lax.cumsum(log_keep, axis=2, reverse=True) - log_keep
    stick_weights = jnp.where(
        usable, jnp.exp(jax.nn.log_sigmoid(scores) + suffix + logsum[:, :, None]), 0.0
    )
    stick_weights = stick_weights.astype(jnp.bfloat16)
    result = result + jnp.einsum(
        "hts,shd->htd", stick_weights, values, preferred_element_type=jnp.float32
    )
    logsum = logsum + jnp.sum(log_keep, axis=2)
    return (result, logsum)


def by_collectives(
    tokens,
    pre_gain,
    w_query_stick,
    w_key_stick,
    w_value_stick,
    w_query_window,
    w_key_window,
    w_value_window,
    stick_bias,
    sinks,
    stick_gain,
    window_gain,
    w_out_stick,
    w_out_window,
    post_gain,
):
    gathered = lax.all_gather(tokens, "tp", axis=1, tiled=True)
    normed = norm_rows(gathered.astype(jnp.float32), pre_gain).astype(jnp.bfloat16)

    def project(weight):
        return jnp.dot(normed, weight, preferred_element_type=jnp.float32).astype(jnp.bfloat16)

    tok_rows = normed.shape[0]
    dev_index = lax.axis_index("sp")
    dev_count = lax.axis_size("sp")
    query_stick = project(w_query_stick)
    stick_heads = query_stick.shape[1] // HEAD_DIM
    queries = query_stick.reshape(tok_rows, stick_heads, HEAD_DIM)
    own_pair = jnp.stack([project(w_key_stick), project(w_value_stick)])
    pair_width = own_pair.shape[2]
    positions = jnp.arange(tok_rows, dtype=jnp.int32)
    initial = (
        jnp.zeros((stick_heads, tok_rows, HEAD_DIM), jnp.float32),
        jnp.zeros((stick_heads, tok_rows), jnp.float32),
    )
    collected = own_pair[None]
    for section_index in range(dev_count.bit_length() - 1):
        arrived = passed_along(collected, "sp", 2**section_index)
        collected = jnp.concatenate([arrived, collected], axis=0)
    per_group = min(dev_count, 8)
    group_count = dev_count // per_group
    grouped = collected.reshape(group_count, per_group, 2, tok_rows, pair_width)
    grouped = grouped.transpose(0, 2, 1, 3, 4).reshape(
        group_count, 2, per_group * tok_rows, pair_width
    )
    first_source = dev_index - (dev_count - 1)
    group_starts = (first_source + jnp.arange(group_count, dtype=jnp.int32) * per_group) * tok_rows
    query_pos = dev_index * tok_rows + positions
    span_offs = jnp.arange(per_group * tok_rows, dtype=jnp.int32)

    def visit_group(carried, inputs):
        key_pair, start_pos = inputs
        key_pos = start_pos + span_offs
        key_mask = (key_pos[None, :] >= 0) & (key_pos[None, :] < query_pos[:, None])
        return (stick_block(queries, key_pair, stick_bias, key_mask, carried), None)

    (stick_sum, _), _ = lax.scan(visit_group, initial, (grouped, group_starts), reverse=True)
    stick_out = (
        stick_sum.transpose(1, 0, 2).reshape(tok_rows, stick_heads * HEAD_DIM).astype(jnp.bfloat16)
    )
    query_window = project(w_query_window)
    window_pair = jnp.stack([project(w_key_window), project(w_value_window)])
    kv_heads = window_pair.shape[2] // HEAD_DIM
    previous = passed_along(window_pair, "sp", 1)
    extended = jnp.concatenate([previous, window_pair], axis=1)
    block_count = tok_rows // WINDOW
    extended = extended.reshape(2, block_count + 1, WINDOW, kv_heads, HEAD_DIM)
    banded = jnp.concatenate([extended[:, :-1], extended[:, 1:]], axis=2)
    q_blocks = query_window.reshape(block_count, WINDOW, kv_heads, GROUP, HEAD_DIM)
    logits = jnp.einsum(
        "nqhgd,nchd->nhgqc", q_blocks, banded[0], preferred_element_type=jnp.float32
    ) * HEAD_DIM ** (-0.5)
    query_offs = jnp.arange(WINDOW, dtype=jnp.int32)[:, None]
    key_offs = jnp.arange(2 * WINDOW, dtype=jnp.int32)[None, :]
    distance = query_offs + WINDOW - key_offs
    key_pos = (
        dev_index * tok_rows
        + jnp.arange(block_count, dtype=jnp.int32)[:, None] * WINDOW
        - WINDOW
        + key_offs
    )
    usable = ((distance >= 0) & (distance < WINDOW))[None] & (key_pos >= 0)[:, None, :]
    logits = jnp.where(usable[:, None, None], logits, -jnp.inf)
    sink_logit = sinks.reshape(kv_heads, GROUP)[None, :, :, None, None]
    row_top = jnp.maximum(jnp.max(logits, axis=-1, keepdims=True), sink_logit)
    weights_exp = jnp.exp(logits - row_top)
    normalizer = jnp.sum(weights_exp, axis=-1, keepdims=True) + jnp.exp(sink_logit - row_top)
    window_weights = (weights_exp / normalizer).astype(jnp.bfloat16)
    window_sum = jnp.einsum(
        "nhgqc,nchd->nqhgd", window_weights, banded[1], preferred_element_type=jnp.float32
    )
    window_out = window_sum.reshape(tok_rows, query_window.shape[1]).astype(jnp.bfloat16)
    stick_float = stick_out.astype(jnp.float32)
    window_float = window_out.astype(jnp.float32)
    squares = lax.psum(
        (jnp.sum(stick_float * stick_float, axis=1), jnp.sum(window_float * window_float, axis=1)),
        "tp",
    )
    stick_normed = (
        stick_float * lax.rsqrt(squares[0][:, None] / (stick_gain.shape[0] * lax.axis_size("tp")) + EPS) * stick_gain
    ).astype(jnp.bfloat16)
    window_normed = (
        window_float * lax.rsqrt(squares[1][:, None] / (window_gain.shape[0] * lax.axis_size("tp")) + EPS) * window_gain
    ).astype(jnp.bfloat16)
    total = jnp.dot(stick_normed, w_out_stick, preferred_element_type=jnp.float32)
    combined = lax.psum_scatter(
        (total + jnp.dot(window_normed, w_out_window, preferred_element_type=jnp.float32)).astype(
            jnp.bfloat16
        ),
        "tp",
        scatter_dimension=0,
        tiled=True,
    ).astype(jnp.float32)
    combined = rounded(combined)
    return norm_rows(combined, post_gain).astype(jnp.bfloat16)


def solution(mesh):
    in_specs = (
        P("sp", "tp"),
        P(),
        P(None, "tp"),
        P(None, "tp"),
        P(None, "tp"),
        P(None, "tp"),
        P(None, "tp"),
        P(None, "tp"),
        P("tp"),
        P("tp"),
        P("tp"),
        P("tp"),
        P("tp", None),
        P("tp", None),
        P(),
    )
    n_sp, n_tp = mesh.shape["sp"], mesh.shape["tp"]

    def shards(*args):
        heads = args[2].shape[1] // HEAD_DIM
        if n_tp == 2 and n_tp * heads == n_sp and args[0].shape[0] == WINDOW and n_sp % 4 == 0:
            return one_kernel(n_sp, *args)
        return by_collectives(*args)

    return jax.shard_map(
        shards,
        mesh=mesh,
        in_specs=in_specs,
        out_specs=P(("sp", "tp"), None),
        check_vma=False,
    )
```

```python
import functools

import jax
import jax.numpy as jnp
from jax import lax
from jax.experimental import pallas as pl
from jax.experimental.pallas import tpu as pltpu
from jax.sharding import PartitionSpec as P

HEAD_DIM = 64
GROUP = 2
WINDOW = 128
EPS = 1e-06
LOG2E = 1.4426950408889634
MESH = pl.DeviceIdType.MESH


class Phases:
    def __init__(self):
        self.scope = None

    def __call__(self, name):
        if self.scope is not None:
            self.scope.__exit__(None, None, None)
            self.scope = None
        if name:
            self.scope = jax.named_scope(name)
            self.scope.__enter__()


def dot(a, b):
    return jnp.dot(a, b, preferred_element_type=jnp.float32)


def dot_t(a, b):
    return lax.dot_general(a, b, (((1,), (1,)), ((), ())), preferred_element_type=jnp.float32)


TILE_BLOCKS = 2
AHEAD = 4
OWN_LAST = 1
PREV_AT = 1
UP_AT = 0
DOWN_AT = 0
HLB_FIRST = False


def kernel(
    n_sp,
    tokens, pre_gain_in, wqs, wks, wvs, wqw, wkw, wvw, bias_in, sinks_in, sgain_in, wgain_in, wos, wow,
    post_gain_in, out,
    pre_gain, bias, sinks, sgain, wgain, post_gain, x, xg, vqs, vks, vvs, vqw, vkw, vvw, vos, vow,
    proj, kv_send, kv_all, q_pad, acc, mass,
    qw, kvw, kvw_prev, w_out_buf, o_send, o_recv, late_send, late_recv, s_out_buf,
    sq_send, sq_recv, total_w, comb, c_send, c_recv, wc_send, wc_recv,
    w_sem, small_sem, tok_sem, x_ss, x_rs, kv_ss, kv_rs, far_ss,
    p_ss, p_rs, o_ss, o_rs, late_ss, late_rs, sq_ss, sq_rs, c_ss, c_rs, wc_ss, wc_rs, hello, all_in,
):
    bf = jnp.bfloat16
    f32 = jnp.float32
    s = lax.axis_index("sp")
    t = lax.axis_index("tp")
    other = 1 - t
    rows, feat_half = tokens.shape
    feats = 2 * feat_half
    half = rows // 2
    hd = HEAD_DIM
    heads = wqs.shape[1] // hd
    kv_heads = wkw.shape[1] // hd
    sw = wqs.shape[1]
    blocks_in_zone = heads // 2
    ph = Phases()
    ph("a_entry")

    tok_load = pltpu.make_async_copy(tokens, x.at[0], tok_sem)
    tok_load.start()
    smalls = [
        pltpu.make_async_copy(src, dst, small_sem.at[n])
        for n, (src, dst) in enumerate(
            [(bias_in, bias), (pre_gain_in, pre_gain), (sinks_in, sinks), (sgain_in, sgain),
             (wgain_in, wgain), (post_gain_in, post_gain)]
        )
    ]
    for load in smalls:
        load.start()

    barrier = pltpu.get_barrier_semaphore()
    partner = {"sp": s, "tp": other}

    @pl.when(t == 0)
    def _():
        pl.semaphore_signal(barrier, inc=1, device_id=partner, device_id_type=MESH)

    def greet(k, carry):
        pl.semaphore_signal(
            barrier, inc=1, device_id={"sp": lax.rem(s + k, n_sp), "tp": 0}, device_id_type=MESH
        )
        return carry

    lax.fori_loop(1, n_sp, greet, 0, unroll=True)

    own_rows = pl.ds(pl.multiple_of(t * feat_half, feat_half), feat_half)
    other_rows = pl.ds(pl.multiple_of(other * feat_half, feat_half), feat_half)
    loads = {}
    for n, (name, src, dst) in enumerate(
        [("ks", wks, vks), ("vs", wvs, vvs), ("qs", wqs, vqs), ("kw", wkw, vkw), ("vw", wvw, vvw), ("qw", wqw, vqw)]
    ):
        loads[name] = [
            pltpu.make_async_copy(src.at[own_rows], dst.at[0], w_sem.at[2 * n]),
            pltpu.make_async_copy(src.at[other_rows], dst.at[1], w_sem.at[2 * n + 1]),
        ]
    l_ow = pltpu.make_async_copy(wow, vow, w_sem.at[12])
    l_os = pltpu.make_async_copy(wos, vos, w_sem.at[13])

    for part_of in range(2):
        for name in ("ks", "vs", "qs"):
            loads[name][part_of].start()
    ph("b_hello")

    @pl.when(t == 1)
    def _():
        pl.semaphore_wait(barrier, 1)
        pl.semaphore_signal(hello, inc=1, device_id=partner, device_id_type=MESH)

    @pl.when(t == 0)
    def _():
        pl.semaphore_wait(hello, 1)

    def to_partner(src, dst, ss, rs):
        return pltpu.make_async_remote_copy(
            src_ref=src, dst_ref=dst, send_sem=ss, recv_sem=rs,
            device_id={"sp": s, "tp": other}, device_id_type=MESH,
        )

    ph("b_tokwait")
    tok_load.wait()
    x_copy = to_partner(x.at[0], x.at[1], x_ss, x_rs)
    x_copy.start()
    for load in smalls:
        load.wait()

    ph("c_gain")
    gain = pre_gain[...].reshape(1, feats)
    gains = [
        jnp.where(t == 0, gain[:, :feat_half], gain[:, feat_half:]),
        jnp.where(t == 0, gain[:, feat_half:], gain[:, :feat_half]),
    ]

    def scaled(n):
        value = x[n].astype(f32)
        xg[n] = (value * gains[n]).astype(bf)
        return jnp.sum(value * value, axis=1, keepdims=True)

    squares = scaled(0)

    ph("e_own")
    for n, (name, w) in enumerate([("ks", vks), ("vs", vvs), ("qs", vqs)]):
        loads[name][0].wait()
        proj[n] = dot(xg[0], w[0])
    for name in ("kw", "vw", "qw"):
        for load in loads[name]:
            load.start()
    ph("f_xwait")
    x_copy.wait_recv()
    ph("g_kvq")
    for name in ("ks", "vs", "qs"):
        loads[name][1].wait()
    inv = lax.rsqrt((squares + scaled(1)) * (1.0 / feats) + EPS)
    keys = (proj[0] + dot(xg[1], vks[1])) * inv
    values = (proj[1] + dot(xg[1], vvs[1])) * inv
    for i in range(heads):
        cols = slice(i * hd, (i + 1) * hd)
        kv_send[i, :rows] = jnp.concatenate([keys[:, cols], values[:, cols]], axis=1).astype(bf)
    queries = (proj[2] + dot(xg[1], vqs[1])) * (inv * (LOG2E * hd**-0.5))
    for i in range(heads):
        cols = slice(i * hd, (i + 1) * hd)
        kv_send[i, rows:] = jnp.concatenate([queries[:half, cols], queries[half:, cols]], axis=1).astype(bf)

    ph("h_barrier")

    @pl.when(t == 0)
    def _():
        pl.semaphore_wait(barrier, 2 * (n_sp - 1))
        pl.semaphore_signal(all_in, inc=1, device_id=partner, device_id_type=MESH)

    @pl.when(t == 1)
    def _():
        pl.semaphore_wait(all_in, 1)

    ph("i_scatter")
    side = s // heads
    slot = lax.rem(s, heads)
    plane = lax.rem(s // blocks_in_zone, 2)
    first = side * heads
    above = lax.rem(slot + t, 2) == 0
    below = jnp.logical_not(above)
    lower = side == 0
    upper = side == 1

    across = [n // 2 + (n % 2) * (heads // 4) for n in range(heads // 2)]

    def far_copy(m, part_of):
        i = 2 * m + lax.rem(t + side, 2)
        return pltpu.make_async_remote_copy(
            src_ref=kv_send.at[i, part_of], dst_ref=kv_all.at[s, part_of], send_sem=far_ss.at[m],
            recv_sem=kv_rs.at[s], device_id={"sp": (1 - side) * heads + i, "tp": t}, device_id_type=MESH,
        )

    keys_part, queries_part = slice(0, rows), slice(rows, rows + half)

    def near_copy(i):
        return pltpu.make_async_remote_copy(
            src_ref=kv_send.at[i], dst_ref=kv_all.at[s], send_sem=kv_ss.at[i],
            recv_sem=kv_rs.at[s], device_id={"sp": first + i, "tp": t}, device_id_type=MESH,
        )

    def send_far(moment):
        if moment == UP_AT:
            @pl.when(lower)
            def _():
                for m in across:
                    far_copy(m, keys_part).start()

        if moment == DOWN_AT:
            @pl.when(upper)
            def _():
                for m in across:
                    far_copy(m, queries_part).start()

    def send_near(n):
        i = lax.rem(n + (OWN_LAST - plane) * (OWN_LAST * 2 - 1) * (heads // 2), heads)

        @pl.when(i == slot)
        def _():
            pltpu.make_async_copy(kv_send.at[i], kv_all.at[s], kv_rs.at[s]).start()

        @pl.when(i != slot)
        def _():
            near_copy(i).start()

    for n in range(heads):
        send_near(n)
    send_far(0)

    ph("j_wproj")
    l_ow.start()
    l_os.start()
    for load in loads["kw"] + loads["vw"]:
        load.wait()
    kvw[:, : kv_heads * hd] = ((dot(xg[0], vkw[0]) + dot(xg[1], vkw[1])) * inv).astype(bf)
    kvw[:, kv_heads * hd :] = ((dot(xg[0], vvw[0]) + dot(xg[1], vvw[1])) * inv).astype(bf)
    prev_copy = lambda to: pltpu.make_async_remote_copy(
        src_ref=kvw, dst_ref=kvw_prev, send_sem=p_ss, recv_sem=p_rs,
        device_id={"sp": to, "tp": t}, device_id_type=MESH,
    )

    for load in loads["qw"]:
        load.wait()
    qw[...] = ((dot(xg[0], vqw[0]) + dot(xg[1], vqw[1])) * inv).astype(bf)

    send_far(1)

    def send_prev():
        @pl.when(s < n_sp - 1)
        def _():
            prev_copy(s + 1).start()

    ph("k_misc")
    head_bias = bias[slot] * LOG2E
    kt = TILE_BLOCKS * rows
    zone = blocks_in_zone * rows
    later = (
        lax.broadcasted_iota(jnp.int32, (kt, kt), 0) > lax.broadcasted_iota(jnp.int32, (kt, kt), 1)
    ).astype(bf)
    before = lax.broadcasted_iota(jnp.int32, (kt, kt), 1) < lax.broadcasted_iota(jnp.int32, (kt, kt), 0)

    def landed(src, ref):
        pltpu.make_async_remote_copy(
            src_ref=ref, dst_ref=ref, send_sem=kv_ss.at[0], recv_sem=kv_rs.at[src],
            device_id=partner, device_id_type=MESH,
        ).wait_recv()

    def take_q(k):
        slab = kv_all[k, rows:].astype(f32)
        zero = jnp.zeros((half, hd), f32)
        both = jnp.concatenate(
            [jnp.concatenate([slab[:, :hd], zero], axis=1), jnp.concatenate([slab[:, hd:], zero], axis=1)], axis=0
        )
        q_pad[pl.ds(pl.multiple_of(k * rows, rows), rows), :] = both.astype(bf)

    def weigh(tiles):
        drops, holds = [], []
        for qs, kv, masked in tiles:
            z = dot_t(qs, kv) + head_bias
            pos = jnp.maximum(z, 0.0)
            drop = pos + jnp.log2(1.0 + jnp.exp2(z - pos - pos))
            hold = z - drop
            if masked:
                drop_top = jnp.where(before, drop[:kt], 0.0)
                hold_top = jnp.where(before, hold[:kt], -jnp.inf)
                if drop.shape[0] == kt:
                    drop, hold = drop_top, hold_top
                else:
                    drop = jnp.concatenate([drop_top, drop[kt:]], axis=0)
                    hold = jnp.concatenate([hold_top, hold[kt:]], axis=0)
            drops.append(drop)
            holds.append(hold)
        suffixes = [dot(drop.astype(bf), later) for drop in drops]
        results = []
        for (_, kv, _), drop, hold, suffix in zip(tiles, drops, holds, suffixes):
            total = jnp.broadcast_to(suffix[:, :1] + drop[:, :1], (drop.shape[0], 2 * hd))
            results.append((dot(jnp.exp2(hold - suffix).astype(bf), kv), total))
        return results

    def keys_of(c, n):
        return kv_all[pl.ds(blocks_in_zone * c + TILE_BLOCKS * n, TILE_BLOCKS), :rows].reshape(kt, 2 * hd)

    def rows_of(c, count):
        return pl.ds(pl.multiple_of(c * zone, zone), count)

    def add(at, result):
        passed = mass[at]
        acc[at] = acc[at] + jnp.exp2(-passed) * result[0]
        mass[at] = passed + result[1]

    def own_pairs(c):
        at = rows_of(c, zone)
        qs = q_pad[at]
        (res1, total1), (res0, total0) = weigh([(qs[kt:], keys_of(c, 1), True), (qs, keys_of(c, 0), True)])
        acc[at] = jnp.concatenate([res0[:kt], res1 + jnp.exp2(-total1) * res0[kt:]], axis=0)
        mass[at] = jnp.concatenate([total0[:kt], total1 + total0[kt:]], axis=0)

    def cross_pairs(qc, kc, fresh):
        at = rows_of(qc, zone)
        qs = q_pad[at]
        one, two_ = weigh([(qs, keys_of(kc, 1), False), (qs, keys_of(kc, 0), False)])
        if fresh:
            acc[at] = one[0] + jnp.exp2(-one[1]) * two_[0]
            mass[at] = one[1] + two_[1]
        else:
            add(at, one)
            add(at, two_)

    def o_copy(k):
        return pltpu.make_async_remote_copy(
            src_ref=o_send.at[k], dst_ref=o_recv.at[slot], send_sem=o_ss.at[k], recv_sem=o_rs.at[slot],
            device_id={"sp": k, "tp": t}, device_id_type=MESH,
        )

    def give(zones):
        blocks = [blocks_in_zone * c + b for c in zones for b in range(blocks_in_zone)]
        for k in blocks:
            value = acc[pl.ds(pl.multiple_of(k * rows, rows), rows), :][:, hd:]
            o_send[k] = jnp.concatenate([value[:half], value[half:]], axis=1).astype(bf)
        for k in blocks:

            @pl.when(k == s)
            def _():
                pltpu.make_async_copy(o_send.at[k], o_recv.at[slot], o_rs.at[slot]).start()

            @pl.when(k != s)
            def _():
                o_copy(k).start()

    def late_copy(j):
        return pltpu.make_async_remote_copy(
            src_ref=late_send.at[j], dst_ref=late_recv.at[slot // 2], send_sem=late_ss.at[j],
            recv_sem=late_rs.at[slot // 2], device_id={"sp": first + j, "tp": t}, device_id_type=MESH,
        )

    def give_late():
        low_lanes = lax.broadcasted_iota(jnp.int32, (rows, 2 * hd), 1) < hd
        for j in range(heads):
            at = pl.ds(pl.multiple_of((first + j) * rows, rows), rows)
            value = jnp.where(low_lanes, jnp.exp2(-mass[at]), acc[at])
            swapped = jnp.concatenate([value[:, hd:], value[:, :hd]], axis=1)
            late_send[j] = jnp.where(lax.rem(slot, 2) == 1, value, swapped).astype(bf)
        for j in range(heads):

            @pl.when(j == slot)
            def _():
                pltpu.make_async_copy(late_send.at[j], late_recv.at[slot // 2], late_rs.at[slot // 2]).start()

            @pl.when(j != slot)
            def _():
                late_copy(j).start()

    own_zone = 2 * side + plane
    next_zone = 2 * side + 1 - plane

    def arrive(c):
        for b in range(blocks_in_zone):
            landed(blocks_in_zone * c + b, kv_all.at[blocks_in_zone * c + b])
        for b in range(blocks_in_zone):
            take_q(blocks_in_zone * c + b)

    ph("l_arrive0")
    arrive(own_zone)
    send_far(2)
    if PREV_AT == 0:
        send_prev()
    ph("l_own0")
    own_pairs(own_zone)
    ph("m_arrive1")
    arrive(next_zone)
    send_far(3)
    if PREV_AT == 1:
        send_prev()
    def lower_pairs():
        @pl.when(jnp.logical_and(lower, below))
        def _():
            for c in (2, 3):
                for b in range(blocks_in_zone):
                    landed(blocks_in_zone * c + b, kv_all.at[blocks_in_zone * c + b, rows:])
                for b in range(blocks_in_zone):
                    take_q(blocks_in_zone * c + b)
                cross_pairs(c, 1, True)
                cross_pairs(c, 0, False)
                give([c])

    ph("m_hlb")
    if HLB_FIRST:
        lower_pairs()
    ph("m_own1")
    own_pairs(next_zone)
    cross_pairs(2 * side + 1, 2 * side, False)
    ph("m_give")

    @pl.when(lower)
    def _():
        give(range(2))

    @pl.when(jnp.logical_and(upper, below))
    def _():
        give_late()

    ph("m_hla")
    if not HLB_FIRST:
        lower_pairs()

    @pl.when(jnp.logical_and(upper, above))
    def _():
        at = rows_of(2, 2 * zone)
        for c in (1, 0):
            for b in range(blocks_in_zone):
                landed(blocks_in_zone * c + b, kv_all.at[blocks_in_zone * c + b, :rows])
            for n in (1, 0):
                add(at, weigh([(q_pad[at], keys_of(c, n), False)])[0])
        give((2, 3))

    ph("n_prev")

    @pl.when(s == 0)
    def _():
        kvw_prev[...] = jnp.zeros_like(kvw_prev)

    @pl.when(s > 0)
    def _():
        prev_copy(s - 1).wait_recv()

    ph("o_window")
    two = 2 * rows
    r_iota = lax.broadcasted_iota(jnp.int32, (two, two), 0)
    c_iota = lax.broadcasted_iota(jnp.int32, (two, two), 1)
    dist = lax.rem(r_iota, rows) + rows - c_iota
    in_window = (dist >= 0) & (dist < WINDOW) & ((c_iota >= rows) | (s > 0))
    first_rows = lax.broadcasted_iota(jnp.int32, (two, 1), 0) < rows
    for g in range(kv_heads):
        cols = slice(g * hd, (g + 1) * hd)
        v_cols = slice((kv_heads + g) * hd, (kv_heads + g + 1) * hd)
        kk = jnp.concatenate([kvw_prev[:, cols], kvw[:, cols]], axis=0)
        vv = jnp.concatenate([kvw_prev[:, v_cols], kvw[:, v_cols]], axis=0)
        base = g * GROUP * hd
        qq = jnp.concatenate(
            [qw[:, base : base + hd], qw[:, base + hd : base + 2 * hd]], axis=0
        )
        logits = jnp.where(in_window, dot_t(qq, kk) * hd**-0.5, -jnp.inf)
        sink = jnp.where(first_rows, sinks[GROUP * g], sinks[GROUP * g + 1])
        top = jnp.maximum(jnp.max(logits, axis=1, keepdims=True), sink)
        grown = jnp.exp(logits - top)
        total = jnp.sum(grown, axis=1, keepdims=True) + jnp.exp(sink - top)
        weights = (grown / total).astype(bf)
        res = dot(weights, vv)
        w_out_buf[:, base : base + 2 * hd] = jnp.concatenate([res[:rows], res[rows:]], axis=1).astype(bf)

    ph("p_sqw")
    theirs = pl.ds(pl.multiple_of(other * half, half), half)
    mine = pl.ds(pl.multiple_of(t * half, half), half)
    n_cut = c_send.shape[0]
    cut = feats // n_cut

    def squares_to_partner(n, squared):
        sq_send[n] = jnp.broadcast_to(jnp.sum(squared, axis=1, keepdims=True), (rows, 128))
        copy = to_partner(sq_send.at[n, theirs], sq_recv.at[n], sq_ss.at[n], sq_rs.at[n])
        copy.start()
        return copy

    def halves_to_partner(left, weights, total, send, recv, ss, rs):
        copies = []

        def give_half(n):
            send[n] = total[theirs, n * cut : (n + 1) * cut].astype(bf)
            copy = to_partner(send.at[n], recv.at[n], ss.at[n], rs.at[n])
            copy.start()
            copies.append(copy)

        for n in range(n_cut):
            cols = slice(n * cut, (n + 1) * cut)
            total[:, cols] = dot(left, weights[:, cols])
            if n >= AHEAD:
                give_half(n - AHEAD)
        for n in range(n_cut - AHEAD, n_cut):
            give_half(n)
        return copies

    wf = w_out_buf[...].astype(f32)
    sq_w = squares_to_partner(0, wf * wf)
    l_ow.wait()
    w_copies = halves_to_partner((wf * wgain[...].reshape(1, sw)).astype(bf), vow, total_w, wc_send, wc_recv, wc_ss, wc_rs)
    ph("r_takeo")

    for i in range(heads):
        pltpu.make_async_remote_copy(
            src_ref=o_send.at[0], dst_ref=o_recv.at[i], send_sem=o_ss.at[0],
            recv_sem=o_rs.at[i], device_id=partner, device_id_type=MESH,
        ).wait_recv()
    ph("s_sout")
    for j in range(heads // 2):
        one = o_recv[2 * j].astype(f32)
        two_ = o_recv[2 * j + 1].astype(f32)
        cols = slice(2 * j * hd, 2 * (j + 1) * hd)
        s_out_buf[:half, cols] = jnp.concatenate([one[:, :hd], two_[:, :hd]], axis=1)
        s_out_buf[half:, cols] = jnp.concatenate([one[:, hd:], two_[:, hd:]], axis=1)

    @pl.when(upper)
    def _():
        in_late = (lax.broadcasted_iota(jnp.int32, (rows, 2 * hd), 1) // hd) == lax.rem(t + 1, 2)
        for j in range(heads // 2):
            pltpu.make_async_remote_copy(
                src_ref=late_send.at[0], dst_ref=late_recv.at[j], send_sem=late_ss.at[0],
                recv_sem=late_rs.at[j], device_id=partner, device_id_type=MESH,
            ).wait_recv()
            cols = slice(2 * j * hd, 2 * (j + 1) * hd)
            early = s_out_buf[:, cols]
            value = late_recv[j].astype(f32)
            swapped = jnp.concatenate([value[:, hd:], value[:, :hd]], axis=1)
            joined = (value + swapped * early).astype(bf).astype(f32)
            s_out_buf[:, cols] = jnp.where(in_late, joined, early)

    sf = s_out_buf[...]
    sq_s = squares_to_partner(1, sf * sf)
    ph("t_os")
    l_os.wait()
    copies = halves_to_partner((sf * sgain[...].reshape(1, sw)).astype(bf), vos, comb, c_send, c_recv, c_ss, c_rs)
    ph("u_wsum")
    sw_cols = 2.0 * sw
    sq_w.wait_recv()
    inv_w = lax.rsqrt((sq_send[0, mine] + sq_recv[0])[:, :1] / sw_cols + EPS)
    for n in range(n_cut):
        cols = slice(n * cut, (n + 1) * cut)
        w_copies[n].wait_recv()
        total_w[:half, cols] = (total_w[mine, cols] + wc_recv[n].astype(f32)) * inv_w

    ph("w_drain")
    x_copy.wait_send()

    for i in range(heads):
        @pl.when(i != slot)
        def _():
            near_copy(i).wait_send()

    @pl.when(lower)
    def _():
        for m in range(heads // 2):
            far_copy(m, keys_part).wait_send()

    @pl.when(upper)
    def _():
        for m in range(heads // 2):
            far_copy(m, queries_part).wait_send()

    @pl.when(s < n_sp - 1)
    def _():
        prev_copy(s + 1).wait_send()

    gives_low = lower
    gives_high = jnp.logical_or(jnp.logical_and(upper, above), jnp.logical_and(lower, below))
    for k in range(n_sp):
        @pl.when(jnp.logical_and(gives_low if k < heads else gives_high, k != s))
        def _():
            o_copy(k).wait_send()

    @pl.when(jnp.logical_and(upper, below))
    def _():
        for j in range(heads):
            @pl.when(j != slot)
            def _():
                late_copy(j).wait_send()

    sq_w.wait_send()
    sq_s.wait_send()

    ph("x_sqrecv")
    sq_s.wait_recv()
    inv_s = lax.rsqrt((sq_send[1, mine] + sq_recv[1])[:, :1] / sw_cols + EPS)
    ph("x_crecv")
    square = jnp.zeros((half, 1), f32)
    for n in range(n_cut):
        cols = slice(n * cut, (n + 1) * cut)
        copies[n].wait_recv()
        summed = (comb[mine, cols] + c_recv[n].astype(f32)) * inv_s + total_w[:half, cols]
        summed = summed.astype(bf).astype(f32)
        total_w[:half, cols] = summed
        square = square + jnp.sum(summed * summed, axis=1, keepdims=True)
    ph("y_out")
    inv = lax.rsqrt(square / feats + EPS)
    out[...] = (total_w[:half, :] * inv * post_gain[...].reshape(1, feats)).astype(bf)
    for copy in copies + w_copies:
        copy.wait_send()
    ph(None)


def one_kernel(n_sp, *args):
    tokens, pre_gain, wqs, wks, wvs, wqw, wkw, wvw, bias, sinks, sgain, wgain, wos, wow, post_gain = args
    bf = jnp.bfloat16
    f32 = jnp.float32
    rows, feat_half = tokens.shape
    feats = 2 * feat_half
    half = rows // 2
    hd = HEAD_DIM
    heads = wqs.shape[1] // hd
    sw = wqs.shape[1]
    wide = 2 * hd
    kvw_cols = wkw.shape[1] + wvw.shape[1]
    assert 2 * heads == n_sp and rows == WINDOW and heads == 4 * TILE_BLOCKS
    v = pltpu.VMEM
    dma = pltpu.SemaphoreType.DMA
    anywhere = pl.BlockSpec(memory_space=pl.ANY)
    vmem = pl.BlockSpec(memory_space=pltpu.VMEM)
    n_cut = 4
    split = lambda w: v((2, w.shape[0] // 2, w.shape[1]), bf)
    scratch = [
        v(pre_gain.shape, f32), pltpu.SMEM(bias.shape, f32), pltpu.SMEM(sinks.shape, f32),
        v(sgain.shape, f32), v(wgain.shape, f32), v(post_gain.shape, f32),
        v((2, rows, feat_half), bf), v((2, rows, feat_half), bf),
        split(wqs), split(wks), split(wvs), split(wqw), split(wkw), split(wvw), v(wos.shape, bf), v(wow.shape, bf),
        v((3, rows, sw), f32),
        v((heads, rows + half, wide), bf), v((n_sp, rows + half, wide), bf),
        v((n_sp * rows, wide), bf),
        v((n_sp * rows, wide), f32), v((n_sp * rows, wide), f32),
        v((rows, sw), bf), v((rows, kvw_cols), bf), v((rows, kvw_cols), bf), v((rows, sw), bf),
        v((n_sp, half, wide), bf), v((heads, half, wide), bf),
        v((heads, rows, wide), bf), v((heads // 2, rows, wide), bf), v((rows, sw), f32),
        v((2, rows, 128), f32), v((2, half, 128), f32), v((rows, feats), f32), v((rows, feats), f32),
        v((n_cut, half, feats // n_cut), bf), v((n_cut, half, feats // n_cut), bf),
        v((n_cut, half, feats // n_cut), bf), v((n_cut, half, feats // n_cut), bf),
        dma((14,)), dma((6,)), dma, dma, dma, dma((heads,)), dma((n_sp,)), dma((heads // 2,)),
        dma, dma, dma((n_sp,)), dma((heads,)), dma((heads,)), dma((heads // 2,)), dma((2,)), dma((2,)),
        dma((n_cut,)), dma((n_cut,)), dma((n_cut,)), dma((n_cut,)), pltpu.SemaphoreType.REGULAR, pltpu.SemaphoreType.REGULAR,
    ]
    return pl.pallas_call(
        functools.partial(kernel, n_sp),
        out_shape=pltpu.VMEM((half, feats), bf),
        in_specs=[anywhere] * len(args),
        out_specs=vmem,
        scratch_shapes=scratch,
        compiler_params=pltpu.CompilerParams(
            collective_id=0, has_side_effects=True, vmem_limit_bytes=60 * 1024 * 1024
        ),
        name="layer",
    )(*[pltpu.with_memory_space_constraint(a, pltpu.HBM) for a in args])


def passed_along(value, axis, steps):
    count = lax.axis_size(axis)
    initial, last = (max(0, -steps), min(count, count - steps))
    return lax.ppermute(value, axis, [(source, source + steps) for source in range(initial, last)])


def rounded(values):
    return lax.optimization_barrier(values.astype(jnp.bfloat16)).astype(jnp.float32)


def norm_rows(values, gain):
    stats = jnp.mean(values * values, axis=-1, keepdims=True)
    return values * lax.rsqrt(stats + EPS) * gain


def stick_block(queries, key_pair, head_bias, key_mask, carried):
    result, logsum = carried
    head_count = queries.shape[1]
    key_rows = key_pair[0].reshape(key_pair.shape[1], head_count, HEAD_DIM)
    values = key_pair[1].reshape(key_pair.shape[1], head_count, HEAD_DIM)
    scores = jnp.einsum(
        "thd,shd->hts", queries, key_rows, preferred_element_type=jnp.float32
    ) * HEAD_DIM ** (-0.5)
    scores = scores + head_bias[:, None, None]
    usable = key_mask[None]
    log_keep = jnp.where(usable, jax.nn.log_sigmoid(-scores), 0.0)
    suffix = lax.cumsum(log_keep, axis=2, reverse=True) - log_keep
    stick_weights = jnp.where(
        usable, jnp.exp(jax.nn.log_sigmoid(scores) + suffix + logsum[:, :, None]), 0.0
    )
    stick_weights = stick_weights.astype(jnp.bfloat16)
    result = result + jnp.einsum(
        "hts,shd->htd", stick_weights, values, preferred_element_type=jnp.float32
    )
    logsum = logsum + jnp.sum(log_keep, axis=2)
    return (result, logsum)


def by_collectives(
    tokens,
    pre_gain,
    w_query_stick,
    w_key_stick,
    w_value_stick,
    w_query_window,
    w_key_window,
    w_value_window,
    stick_bias,
    sinks,
    stick_gain,
    window_gain,
    w_out_stick,
    w_out_window,
    post_gain,
):
    gathered = lax.all_gather(tokens, "tp", axis=1, tiled=True)
    normed = norm_rows(gathered.astype(jnp.float32), pre_gain).astype(jnp.bfloat16)

    def project(weight):
        return jnp.dot(normed, weight, preferred_element_type=jnp.float32).astype(jnp.bfloat16)

    tok_rows = normed.shape[0]
    dev_index = lax.axis_index("sp")
    dev_count = lax.axis_size("sp")
    query_stick = project(w_query_stick)
    stick_heads = query_stick.shape[1] // HEAD_DIM
    queries = query_stick.reshape(tok_rows, stick_heads, HEAD_DIM)
    own_pair = jnp.stack([project(w_key_stick), project(w_value_stick)])
    pair_width = own_pair.shape[2]
    positions = jnp.arange(tok_rows, dtype=jnp.int32)
    initial = (
        jnp.zeros((stick_heads, tok_rows, HEAD_DIM), jnp.float32),
        jnp.zeros((stick_heads, tok_rows), jnp.float32),
    )
    collected = own_pair[None]
    for section_index in range(dev_count.bit_length() - 1):
        arrived = passed_along(collected, "sp", 2**section_index)
        collected = jnp.concatenate([arrived, collected], axis=0)
    per_group = min(dev_count, 8)
    group_count = dev_count // per_group
    grouped = collected.reshape(group_count, per_group, 2, tok_rows, pair_width)
    grouped = grouped.transpose(0, 2, 1, 3, 4).reshape(
        group_count, 2, per_group * tok_rows, pair_width
    )
    first_source = dev_index - (dev_count - 1)
    group_starts = (first_source + jnp.arange(group_count, dtype=jnp.int32) * per_group) * tok_rows
    query_pos = dev_index * tok_rows + positions
    span_offs = jnp.arange(per_group * tok_rows, dtype=jnp.int32)

    def visit_group(carried, inputs):
        key_pair, start_pos = inputs
        key_pos = start_pos + span_offs
        key_mask = (key_pos[None, :] >= 0) & (key_pos[None, :] < query_pos[:, None])
        return (stick_block(queries, key_pair, stick_bias, key_mask, carried), None)

    (stick_sum, _), _ = lax.scan(visit_group, initial, (grouped, group_starts), reverse=True)
    stick_out = (
        stick_sum.transpose(1, 0, 2).reshape(tok_rows, stick_heads * HEAD_DIM).astype(jnp.bfloat16)
    )
    query_window = project(w_query_window)
    window_pair = jnp.stack([project(w_key_window), project(w_value_window)])
    kv_heads = window_pair.shape[2] // HEAD_DIM
    previous = passed_along(window_pair, "sp", 1)
    extended = jnp.concatenate([previous, window_pair], axis=1)
    block_count = tok_rows // WINDOW
    extended = extended.reshape(2, block_count + 1, WINDOW, kv_heads, HEAD_DIM)
    banded = jnp.concatenate([extended[:, :-1], extended[:, 1:]], axis=2)
    q_blocks = query_window.reshape(block_count, WINDOW, kv_heads, GROUP, HEAD_DIM)
    logits = jnp.einsum(
        "nqhgd,nchd->nhgqc", q_blocks, banded[0], preferred_element_type=jnp.float32
    ) * HEAD_DIM ** (-0.5)
    query_offs = jnp.arange(WINDOW, dtype=jnp.int32)[:, None]
    key_offs = jnp.arange(2 * WINDOW, dtype=jnp.int32)[None, :]
    distance = query_offs + WINDOW - key_offs
    key_pos = (
        dev_index * tok_rows
        + jnp.arange(block_count, dtype=jnp.int32)[:, None] * WINDOW
        - WINDOW
        + key_offs
    )
    usable = ((distance >= 0) & (distance < WINDOW))[None] & (key_pos >= 0)[:, None, :]
    logits = jnp.where(usable[:, None, None], logits, -jnp.inf)
    sink_logit = sinks.reshape(kv_heads, GROUP)[None, :, :, None, None]
    row_top = jnp.maximum(jnp.max(logits, axis=-1, keepdims=True), sink_logit)
    weights_exp = jnp.exp(logits - row_top)
    normalizer = jnp.sum(weights_exp, axis=-1, keepdims=True) + jnp.exp(sink_logit - row_top)
    window_weights = (weights_exp / normalizer).astype(jnp.bfloat16)
    window_sum = jnp.einsum(
        "nhgqc,nchd->nqhgd", window_weights, banded[1], preferred_element_type=jnp.float32
    )
    window_out = window_sum.reshape(tok_rows, query_window.shape[1]).astype(jnp.bfloat16)
    stick_float = stick_out.astype(jnp.float32)
    window_float = window_out.astype(jnp.float32)
    squares = lax.psum(
        (jnp.sum(stick_float * stick_float, axis=1), jnp.sum(window_float * window_float, axis=1)),
        "tp",
    )
    stick_normed = (
        stick_float * lax.rsqrt(squares[0][:, None] / (stick_gain.shape[0] * lax.axis_size("tp")) + EPS) * stick_gain
    ).astype(jnp.bfloat16)
    window_normed = (
        window_float * lax.rsqrt(squares[1][:, None] / (window_gain.shape[0] * lax.axis_size("tp")) + EPS) * window_gain
    ).astype(jnp.bfloat16)
    total = jnp.dot(stick_normed, w_out_stick, preferred_element_type=jnp.float32)
    combined = lax.psum_scatter(
        (total + jnp.dot(window_normed, w_out_window, preferred_element_type=jnp.float32)).astype(
            jnp.bfloat16
        ),
        "tp",
        scatter_dimension=0,
        tiled=True,
    ).astype(jnp.float32)
    combined = rounded(combined)
    return norm_rows(combined, post_gain).astype(jnp.bfloat16)


def solution(mesh):
    in_specs = (
        P("sp", "tp"),
        P(),
        P(None, "tp"),
        P(None, "tp"),
        P(None, "tp"),
        P(None, "tp"),
        P(None, "tp"),
        P(None, "tp"),
        P("tp"),
        P("tp"),
        P("tp"),
        P("tp"),
        P("tp", None),
        P("tp", None),
        P(),
    )
    n_sp, n_tp = mesh.shape["sp"], mesh.shape["tp"]

    def shards(*args):
        heads = args[2].shape[1] // HEAD_DIM
        if n_tp == 2 and n_tp * heads == n_sp and args[0].shape[0] == WINDOW and heads == 4 * TILE_BLOCKS:
            return one_kernel(n_sp, *args)
        return by_collectives(*args)

    return jax.shard_map(
        shards,
        mesh=mesh,
        in_specs=in_specs,
        out_specs=P(("sp", "tp"), None),
        check_vma=False,
    )
```

```python
import functools

import jax
import jax.numpy as jnp
from jax import lax
from jax.experimental import pallas as pl
from jax.experimental.pallas import tpu as pltpu
from jax.sharding import PartitionSpec as P

HEAD_DIM = 64
GROUP = 2
WINDOW = 128
EPS = 1e-06
LOG2E = 1.4426950408889634
MESH = pl.DeviceIdType.MESH


class Phases:
    def __init__(self):
        self.scope = None

    def __call__(self, name):
        if self.scope is not None:
            self.scope.__exit__(None, None, None)
            self.scope = None
        if name:
            self.scope = jax.named_scope(name)
            self.scope.__enter__()


def dot(a, b):
    return jnp.dot(a, b, preferred_element_type=jnp.float32)


def dot_t(a, b):
    return lax.dot_general(a, b, (((1,), (1,)), ((), ())), preferred_element_type=jnp.float32)


TILE_BLOCKS = 2
AHEAD = 2
OWN_LAST = 0
PREV_AT = -1
UP_AT = 0
DOWN_AT = 0
HLB_FIRST = False


def kernel(
    n_sp,
    tokens, pre_gain_in, wqs, wks, wvs, wqw, wkw, wvw, bias_in, sinks_in, sgain_in, wgain_in, wos, wow,
    post_gain_in, out,
    pre_gain, bias, sinks, sgain, wgain, post_gain, x, xg, vqs, vks, vvs, vqw, vkw, vvw, vos, vow,
    proj, kv_send, kv_all, q_pad, acc, mass,
    qw, kvw, kvw_prev, w_out_buf, o_send, o_recv, late_send, late_recv, late_scale, s_out_buf,
    sq_send, sq_recv, total_w, comb, c_send, c_recv, wc_send, wc_recv,
    w_sem, small_sem, tok_sem, x_ss, x_rs, kv_ss, kv_rs, far_ss,
    p_ss, p_rs, o_ss, o_rs, late_ss, late_rs, sq_ss, sq_rs, c_ss, c_rs, wc_ss, wc_rs, hello, all_in,
):
    bf = jnp.bfloat16
    f32 = jnp.float32
    s = lax.axis_index("sp")
    t = lax.axis_index("tp")
    other = 1 - t
    rows, feat_half = tokens.shape
    feats = 2 * feat_half
    half = rows // 2
    hd = HEAD_DIM
    heads = wqs.shape[1] // hd
    kv_heads = wkw.shape[1] // hd
    sw = wqs.shape[1]
    blocks_in_zone = heads // 2
    ph = Phases()
    ph("a_entry")

    tok_load = pltpu.make_async_copy(tokens, x.at[0], tok_sem)
    tok_load.start()
    smalls = [
        pltpu.make_async_copy(src, dst, small_sem.at[n])
        for n, (src, dst) in enumerate(
            [(bias_in, bias), (pre_gain_in, pre_gain), (sinks_in, sinks), (sgain_in, sgain),
             (wgain_in, wgain), (post_gain_in, post_gain)]
        )
    ]
    for load in smalls:
        load.start()

    barrier = pltpu.get_barrier_semaphore()
    partner = {"sp": s, "tp": other}

    @pl.when(t == 0)
    def _():
        pl.semaphore_signal(barrier, inc=1, device_id=partner, device_id_type=MESH)

    def greet(k, carry):
        pl.semaphore_signal(
            barrier, inc=1, device_id={"sp": lax.rem(s + k, n_sp), "tp": 0}, device_id_type=MESH
        )
        return carry

    lax.fori_loop(1, n_sp, greet, 0, unroll=True)

    own_rows = pl.ds(pl.multiple_of(t * feat_half, feat_half), feat_half)
    other_rows = pl.ds(pl.multiple_of(other * feat_half, feat_half), feat_half)
    loads = {}
    for n, (name, src, dst) in enumerate(
        [("ks", wks, vks), ("vs", wvs, vvs), ("qs", wqs, vqs), ("kw", wkw, vkw), ("vw", wvw, vvw), ("qw", wqw, vqw)]
    ):
        loads[name] = [
            pltpu.make_async_copy(src.at[own_rows], dst.at[0], w_sem.at[2 * n]),
            pltpu.make_async_copy(src.at[other_rows], dst.at[1], w_sem.at[2 * n + 1]),
        ]
    l_ow = pltpu.make_async_copy(wow, vow, w_sem.at[12])
    l_os = pltpu.make_async_copy(wos, vos, w_sem.at[13])

    for part_of in range(2):
        for name in ("ks", "vs", "qs"):
            loads[name][part_of].start()
    ph("b_hello")

    @pl.when(t == 1)
    def _():
        pl.semaphore_wait(barrier, 1)
        pl.semaphore_signal(hello, inc=1, device_id=partner, device_id_type=MESH)

    @pl.when(t == 0)
    def _():
        pl.semaphore_wait(hello, 1)

    def to_partner(src, dst, ss, rs):
        return pltpu.make_async_remote_copy(
            src_ref=src, dst_ref=dst, send_sem=ss, recv_sem=rs,
            device_id={"sp": s, "tp": other}, device_id_type=MESH,
        )

    ph("b_tokwait")
    tok_load.wait()
    x_copy = to_partner(x.at[0], x.at[1], x_ss, x_rs)
    x_copy.start()
    for load in smalls:
        load.wait()

    ph("c_gain")
    gain = pre_gain[...].reshape(1, feats)
    gains = [
        jnp.where(t == 0, gain[:, :feat_half], gain[:, feat_half:]),
        jnp.where(t == 0, gain[:, feat_half:], gain[:, :feat_half]),
    ]

    def scaled(n):
        value = x[n].astype(f32)
        xg[n] = (value * gains[n]).astype(bf)
        return jnp.sum(value * value, axis=1, keepdims=True)

    squares = scaled(0)

    ph("e_own")
    for n, (name, w) in enumerate([("ks", vks), ("vs", vvs), ("qs", vqs)]):
        loads[name][0].wait()
        proj[n] = dot(xg[0], w[0])
    for name in ("kw", "vw", "qw"):
        for load in loads[name]:
            load.start()
    ph("f_xwait")
    x_copy.wait_recv()
    ph("g_kvq")
    for name in ("ks", "vs", "qs"):
        loads[name][1].wait()
    inv = lax.rsqrt((squares + scaled(1)) * (1.0 / feats) + EPS)
    keys = (proj[0] + dot(xg[1], vks[1])) * inv
    values = (proj[1] + dot(xg[1], vvs[1])) * inv
    for i in range(heads):
        cols = slice(i * hd, (i + 1) * hd)
        kv_send[i, :rows] = jnp.concatenate([keys[:, cols], values[:, cols]], axis=1).astype(bf)
    queries = (proj[2] + dot(xg[1], vqs[1])) * (inv * (LOG2E * hd**-0.5))
    for i in range(heads):
        cols = slice(i * hd, (i + 1) * hd)
        kv_send[i, rows:] = jnp.concatenate([queries[:half, cols], queries[half:, cols]], axis=1).astype(bf)

    ph("h_barrier")

    @pl.when(t == 0)
    def _():
        pl.semaphore_wait(barrier, 2 * (n_sp - 1))
        pl.semaphore_signal(all_in, inc=1, device_id=partner, device_id_type=MESH)

    @pl.when(t == 1)
    def _():
        pl.semaphore_wait(all_in, 1)

    ph("i_scatter")
    side = s // heads
    slot = lax.rem(s, heads)
    plane = lax.rem(s // blocks_in_zone, 2)
    first = side * heads
    above = lax.rem(slot + t, 2) == 0
    below = jnp.logical_not(above)
    lower = side == 0
    upper = side == 1

    across = [n // 2 + (n % 2) * (heads // 4) for n in range(heads // 2)]

    def far_copy(m, part_of):
        i = 2 * m + lax.rem(t + side, 2)
        return pltpu.make_async_remote_copy(
            src_ref=kv_send.at[i, part_of], dst_ref=kv_all.at[s, part_of], send_sem=far_ss.at[m],
            recv_sem=kv_rs.at[s], device_id={"sp": (1 - side) * heads + i, "tp": t}, device_id_type=MESH,
        )

    keys_part, queries_part = slice(0, rows), slice(rows, rows + half)

    def near_copy(i):
        return pltpu.make_async_remote_copy(
            src_ref=kv_send.at[i], dst_ref=kv_all.at[s], send_sem=kv_ss.at[i],
            recv_sem=kv_rs.at[s], device_id={"sp": first + i, "tp": t}, device_id_type=MESH,
        )

    def send_far(moment):
        if moment == UP_AT:
            @pl.when(lower)
            def _():
                for m in across:
                    far_copy(m, keys_part).start()

        if moment == DOWN_AT:
            @pl.when(upper)
            def _():
                for m in across:
                    far_copy(m, queries_part).start()

    def send_near(n):
        i = lax.rem(n + (OWN_LAST - plane) * (OWN_LAST * 2 - 1) * (heads // 2), heads)

        @pl.when(i == slot)
        def _():
            pltpu.make_async_copy(kv_send.at[i], kv_all.at[s], kv_rs.at[s]).start()

        @pl.when(i != slot)
        def _():
            near_copy(i).start()

    for n in range(heads):
        send_near(n)
    send_far(0)

    ph("j_wproj")
    l_ow.start()
    l_os.start()
    for load in loads["kw"] + loads["vw"]:
        load.wait()
    kvw[:, : kv_heads * hd] = ((dot(xg[0], vkw[0]) + dot(xg[1], vkw[1])) * inv).astype(bf)
    kvw[:, kv_heads * hd :] = ((dot(xg[0], vvw[0]) + dot(xg[1], vvw[1])) * inv).astype(bf)
    prev_copy = lambda to: pltpu.make_async_remote_copy(
        src_ref=kvw, dst_ref=kvw_prev, send_sem=p_ss, recv_sem=p_rs,
        device_id={"sp": to, "tp": t}, device_id_type=MESH,
    )

    for load in loads["qw"]:
        load.wait()
    qw[...] = ((dot(xg[0], vqw[0]) + dot(xg[1], vqw[1])) * inv).astype(bf)

    send_far(1)

    def send_prev():
        @pl.when(s < n_sp - 1)
        def _():
            prev_copy(s + 1).start()

    ph("k_misc")
    head_bias = bias[slot] * LOG2E
    kt = TILE_BLOCKS * rows
    zone = blocks_in_zone * rows
    later = (
        lax.broadcasted_iota(jnp.int32, (kt, kt), 0) > lax.broadcasted_iota(jnp.int32, (kt, kt), 1)
    ).astype(bf)
    before = lax.broadcasted_iota(jnp.int32, (kt, kt), 1) < lax.broadcasted_iota(jnp.int32, (kt, kt), 0)

    def landed(src, ref):
        pltpu.make_async_remote_copy(
            src_ref=ref, dst_ref=ref, send_sem=kv_ss.at[0], recv_sem=kv_rs.at[src],
            device_id=partner, device_id_type=MESH,
        ).wait_recv()

    def take_q(k):
        slab = kv_all[k, rows:].astype(f32)
        zero = jnp.zeros((half, hd), f32)
        both = jnp.concatenate(
            [jnp.concatenate([slab[:, :hd], zero], axis=1), jnp.concatenate([slab[:, hd:], zero], axis=1)], axis=0
        )
        q_pad[pl.ds(pl.multiple_of(k * rows, rows), rows), :] = both.astype(bf)

    def weigh(tiles):
        drops, holds = [], []
        for qs, kv, masked in tiles:
            z = dot_t(qs, kv) + head_bias
            pos = jnp.maximum(z, 0.0)
            drop = pos + jnp.log2(1.0 + jnp.exp2(z - pos - pos))
            hold = z - drop
            if masked:
                drop_top = jnp.where(before, drop[:kt], 0.0)
                hold_top = jnp.where(before, hold[:kt], -jnp.inf)
                if drop.shape[0] == kt:
                    drop, hold = drop_top, hold_top
                else:
                    drop = jnp.concatenate([drop_top, drop[kt:]], axis=0)
                    hold = jnp.concatenate([hold_top, hold[kt:]], axis=0)
            drops.append(drop)
            holds.append(hold)
        suffixes = [dot(drop.astype(bf), later) for drop in drops]
        results = []
        for (_, kv, _), drop, hold, suffix in zip(tiles, drops, holds, suffixes):
            total = jnp.broadcast_to(suffix[:, :1] + drop[:, :1], (drop.shape[0], 2 * hd))
            results.append((dot(jnp.exp2(hold - suffix).astype(bf), kv), total))
        return results

    def keys_of(c, n):
        return kv_all[pl.ds(blocks_in_zone * c + TILE_BLOCKS * n, TILE_BLOCKS), :rows].reshape(kt, 2 * hd)

    def rows_of(c, count):
        return pl.ds(pl.multiple_of(c * zone, zone), count)

    def add(at, result):
        passed = mass[at]
        acc[at] = acc[at] + jnp.exp2(-passed) * result[0]
        mass[at] = passed + result[1]

    def own_pairs(c):
        at = rows_of(c, zone)
        qs = q_pad[at]
        (res1, total1), (res0, total0) = weigh([(qs[kt:], keys_of(c, 1), True), (qs, keys_of(c, 0), True)])
        acc[at] = jnp.concatenate([res0[:kt], res1 + jnp.exp2(-total1) * res0[kt:]], axis=0)
        mass[at] = jnp.concatenate([total0[:kt], total1 + total0[kt:]], axis=0)

    def cross_pairs(qc, kc, fresh):
        at = rows_of(qc, zone)
        qs = q_pad[at]
        one, two_ = weigh([(qs, keys_of(kc, 1), False), (qs, keys_of(kc, 0), False)])
        if fresh:
            acc[at] = one[0] + jnp.exp2(-one[1]) * two_[0]
            mass[at] = one[1] + two_[1]
        else:
            add(at, one)
            add(at, two_)

    def o_copy(k):
        return pltpu.make_async_remote_copy(
            src_ref=o_send.at[k], dst_ref=o_recv.at[slot], send_sem=o_ss.at[k], recv_sem=o_rs.at[slot],
            device_id={"sp": k, "tp": t}, device_id_type=MESH,
        )

    def give(zones):
        blocks = [blocks_in_zone * c + b for c in zones for b in range(blocks_in_zone)]
        for k in blocks:
            value = acc[pl.ds(pl.multiple_of(k * rows, rows), rows), :][:, hd:]
            o_send[k] = jnp.concatenate([value[:half], value[half:]], axis=1).astype(bf)
        for k in blocks:

            @pl.when(k == s)
            def _():
                pltpu.make_async_copy(o_send.at[k], o_recv.at[slot], o_rs.at[slot]).start()

            @pl.when(k != s)
            def _():
                o_copy(k).start()

    def late_copy(j):
        return pltpu.make_async_remote_copy(
            src_ref=late_send.at[j], dst_ref=late_recv.at[slot // 2], send_sem=late_ss.at[j],
            recv_sem=late_rs.at[slot // 2], device_id={"sp": first + j, "tp": t}, device_id_type=MESH,
        )

    def give_late():
        low_lanes = lax.broadcasted_iota(jnp.int32, (rows, 2 * hd), 1) < hd
        for j in range(heads):
            at = pl.ds(pl.multiple_of((first + j) * rows, rows), rows)
            value = jnp.where(low_lanes, jnp.exp2(-mass[at]), acc[at])
            swapped = jnp.concatenate([value[:, hd:], value[:, :hd]], axis=1)
            late_send[j] = jnp.where(lax.rem(slot, 2) == 1, value, swapped).astype(bf)
        for j in range(heads):

            @pl.when(j == slot)
            def _():
                pltpu.make_async_copy(late_send.at[j], late_recv.at[slot // 2], late_rs.at[slot // 2]).start()

            @pl.when(j != slot)
            def _():
                late_copy(j).start()

    own_zone = 2 * side + plane
    next_zone = 2 * side + 1 - plane

    def arrive(c):
        for b in range(blocks_in_zone):
            landed(blocks_in_zone * c + b, kv_all.at[blocks_in_zone * c + b])
        for b in range(blocks_in_zone):
            take_q(blocks_in_zone * c + b)

    if PREV_AT < 0:
        for b in range(blocks_in_zone if PREV_AT == -1 else heads):
            i = b + (plane * blocks_in_zone if PREV_AT == -1 else 0)

            @pl.when(i != slot)
            def _():
                near_copy(i).wait_send()

        send_prev()
    ph("l_arrive0")
    arrive(own_zone)
    send_far(2)
    if PREV_AT == 0:
        send_prev()
    ph("l_own0")
    own_pairs(own_zone)
    ph("m_arrive1")
    arrive(next_zone)
    send_far(3)
    if PREV_AT == 1:
        send_prev()
    def lower_pairs():
        @pl.when(jnp.logical_and(lower, below))
        def _():
            for c in (2, 3):
                for b in range(blocks_in_zone):
                    landed(blocks_in_zone * c + b, kv_all.at[blocks_in_zone * c + b, rows:])
                for b in range(blocks_in_zone):
                    take_q(blocks_in_zone * c + b)
                cross_pairs(c, 1, True)
                cross_pairs(c, 0, False)
                give([c])

    ph("m_hlb")
    if HLB_FIRST:
        lower_pairs()
    ph("m_own1")
    own_pairs(next_zone)
    cross_pairs(2 * side + 1, 2 * side, False)
    ph("m_give")

    @pl.when(lower)
    def _():
        give(range(2))

    @pl.when(jnp.logical_and(upper, below))
    def _():
        give_late()

    ph("m_hla")
    if not HLB_FIRST:
        lower_pairs()

    @pl.when(jnp.logical_and(upper, above))
    def _():
        at = rows_of(2, 2 * zone)
        for c in (1, 0):
            for b in range(blocks_in_zone):
                landed(blocks_in_zone * c + b, kv_all.at[blocks_in_zone * c + b, :rows])
            for n in (1, 0):
                add(at, weigh([(q_pad[at], keys_of(c, n), False)])[0])
        give((2, 3))

    ph("n_prev")

    @pl.when(s == 0)
    def _():
        kvw_prev[...] = jnp.zeros_like(kvw_prev)

    @pl.when(s > 0)
    def _():
        prev_copy(s - 1).wait_recv()

    ph("o_window")
    two = 2 * rows
    r_iota = lax.broadcasted_iota(jnp.int32, (two, two), 0)
    c_iota = lax.broadcasted_iota(jnp.int32, (two, two), 1)
    dist = lax.rem(r_iota, rows) + rows - c_iota
    in_window = (dist >= 0) & (dist < WINDOW) & ((c_iota >= rows) | (s > 0))
    first_rows = lax.broadcasted_iota(jnp.int32, (two, 1), 0) < rows
    for g in range(kv_heads):
        cols = slice(g * hd, (g + 1) * hd)
        v_cols = slice((kv_heads + g) * hd, (kv_heads + g + 1) * hd)
        kk = jnp.concatenate([kvw_prev[:, cols], kvw[:, cols]], axis=0)
        vv = jnp.concatenate([kvw_prev[:, v_cols], kvw[:, v_cols]], axis=0)
        base = g * GROUP * hd
        qq = jnp.concatenate(
            [qw[:, base : base + hd], qw[:, base + hd : base + 2 * hd]], axis=0
        )
        logits = jnp.where(in_window, dot_t(qq, kk) * hd**-0.5, -jnp.inf)
        sink = jnp.where(first_rows, sinks[GROUP * g], sinks[GROUP * g + 1])
        top = jnp.maximum(jnp.max(logits, axis=1, keepdims=True), sink)
        grown = jnp.exp(logits - top)
        total = jnp.sum(grown, axis=1, keepdims=True) + jnp.exp(sink - top)
        weights = (grown / total).astype(bf)
        res = dot(weights, vv)
        w_out_buf[:, base : base + 2 * hd] = jnp.concatenate([res[:rows], res[rows:]], axis=1).astype(bf)

    ph("p_sqw")
    theirs = pl.ds(pl.multiple_of(other * half, half), half)
    mine = pl.ds(pl.multiple_of(t * half, half), half)
    n_cut = c_send.shape[0]
    cut = feats // n_cut

    def squares_to_partner(n, squared):
        sq_send[n] = jnp.broadcast_to(jnp.sum(squared, axis=1, keepdims=True), (rows, 128))
        copy = to_partner(sq_send.at[n, theirs], sq_recv.at[n], sq_ss.at[n], sq_rs.at[n])
        copy.start()
        return copy

    def halves_to_partner(left, weights, total, send, recv, ss, rs):
        copies = []

        def give_half(n):
            send[n] = total[theirs, n * cut : (n + 1) * cut].astype(bf)
            copy = to_partner(send.at[n], recv.at[n], ss.at[n], rs.at[n])
            copy.start()
            copies.append(copy)

        for n in range(n_cut):
            cols = slice(n * cut, (n + 1) * cut)
            total[:, cols] = dot(left, weights[:, cols])
            if n >= AHEAD:
                give_half(n - AHEAD)
        for n in range(n_cut - AHEAD, n_cut):
            give_half(n)
        return copies

    wf = w_out_buf[...].astype(f32)
    sq_w = squares_to_partner(0, wf * wf)
    l_ow.wait()
    w_copies = halves_to_partner((wf * wgain[...].reshape(1, sw)).astype(bf), vow, total_w, wc_send, wc_recv, wc_ss, wc_rs)
    ph("q_late")

    @pl.when(lower)
    def _():
        s_out_buf[...] = jnp.zeros_like(s_out_buf)
        late_scale[...] = jnp.ones_like(late_scale)

    @pl.when(upper)
    def _():
        in_late = (lax.broadcasted_iota(jnp.int32, (rows, 2 * hd), 1) // hd) == lax.rem(t + 1, 2)
        for j in range(heads // 2):
            pltpu.make_async_remote_copy(
                src_ref=late_send.at[0], dst_ref=late_recv.at[j], send_sem=late_ss.at[0],
                recv_sem=late_rs.at[j], device_id=partner, device_id_type=MESH,
            ).wait_recv()
        for j in range(heads // 2):
            cols = slice(2 * j * hd, 2 * (j + 1) * hd)
            value = late_recv[j].astype(f32)
            swapped = jnp.concatenate([value[:, hd:], value[:, :hd]], axis=1)
            s_out_buf[:, cols] = jnp.where(in_late, value, 0.0)
            late_scale[:, cols] = jnp.where(in_late, swapped, 1.0)

    ph("r_takeo")

    for i in range(heads):
        pltpu.make_async_remote_copy(
            src_ref=o_send.at[0], dst_ref=o_recv.at[i], send_sem=o_ss.at[0],
            recv_sem=o_rs.at[i], device_id=partner, device_id_type=MESH,
        ).wait_recv()
    ph("s_sout")
    for j in range(heads // 2):
        one = o_recv[2 * j].astype(f32)
        two_ = o_recv[2 * j + 1].astype(f32)
        cols = slice(2 * j * hd, 2 * (j + 1) * hd)
        pair = jnp.concatenate(
            [
                jnp.concatenate([one[:, :hd], two_[:, :hd]], axis=1),
                jnp.concatenate([one[:, hd:], two_[:, hd:]], axis=1),
            ],
            axis=0,
        )
        s_out_buf[:, cols] = (s_out_buf[:, cols] + late_scale[:, cols] * pair).astype(bf).astype(f32)

    sf = s_out_buf[...]
    sq_s = squares_to_partner(1, sf * sf)
    ph("t_os")
    l_os.wait()
    copies = halves_to_partner((sf * sgain[...].reshape(1, sw)).astype(bf), vos, comb, c_send, c_recv, c_ss, c_rs)
    ph("u_wsum")
    sw_cols = 2.0 * sw
    sq_w.wait_recv()
    inv_w = lax.rsqrt((sq_send[0, mine] + sq_recv[0])[:, :1] / sw_cols + EPS)
    for n in range(n_cut):
        cols = slice(n * cut, (n + 1) * cut)
        w_copies[n].wait_recv()
        total_w[:half, cols] = (total_w[mine, cols] + wc_recv[n].astype(f32)) * inv_w

    ph("w_drain")
    x_copy.wait_send()

    for b in range(heads if PREV_AT >= 0 else blocks_in_zone if PREV_AT == -1 else 0):
        i = b if PREV_AT >= 0 else b + (1 - plane) * blocks_in_zone

        @pl.when(i != slot)
        def _():
            near_copy(i).wait_send()

    @pl.when(lower)
    def _():
        for m in range(heads // 2):
            far_copy(m, keys_part).wait_send()

    @pl.when(upper)
    def _():
        for m in range(heads // 2):
            far_copy(m, queries_part).wait_send()

    @pl.when(s < n_sp - 1)
    def _():
        prev_copy(s + 1).wait_send()

    gives_low = lower
    gives_high = jnp.logical_or(jnp.logical_and(upper, above), jnp.logical_and(lower, below))
    for k in range(n_sp):
        @pl.when(jnp.logical_and(gives_low if k < heads else gives_high, k != s))
        def _():
            o_copy(k).wait_send()

    @pl.when(jnp.logical_and(upper, below))
    def _():
        for j in range(heads):
            @pl.when(j != slot)
            def _():
                late_copy(j).wait_send()

    sq_w.wait_send()
    sq_s.wait_send()

    ph("x_sqrecv")
    sq_s.wait_recv()
    inv_s = lax.rsqrt((sq_send[1, mine] + sq_recv[1])[:, :1] / sw_cols + EPS)
    ph("x_crecv")
    square = jnp.zeros((half, 1), f32)
    for n in range(n_cut):
        cols = slice(n * cut, (n + 1) * cut)
        copies[n].wait_recv()
        summed = (comb[mine, cols] + c_recv[n].astype(f32)) * inv_s + total_w[:half, cols]
        summed = summed.astype(bf).astype(f32)
        total_w[:half, cols] = summed
        square = square + jnp.sum(summed * summed, axis=1, keepdims=True)
    ph("y_out")
    inv = lax.rsqrt(square / feats + EPS)
    out[...] = (total_w[:half, :] * inv * post_gain[...].reshape(1, feats)).astype(bf)
    for copy in copies + w_copies:
        copy.wait_send()
    ph(None)


def one_kernel(n_sp, *args):
    tokens, pre_gain, wqs, wks, wvs, wqw, wkw, wvw, bias, sinks, sgain, wgain, wos, wow, post_gain = args
    bf = jnp.bfloat16
    f32 = jnp.float32
    rows, feat_half = tokens.shape
    feats = 2 * feat_half
    half = rows // 2
    hd = HEAD_DIM
    heads = wqs.shape[1] // hd
    sw = wqs.shape[1]
    wide = 2 * hd
    kvw_cols = wkw.shape[1] + wvw.shape[1]
    assert 2 * heads == n_sp and rows == WINDOW and heads == 4 * TILE_BLOCKS
    v = pltpu.VMEM
    dma = pltpu.SemaphoreType.DMA
    anywhere = pl.BlockSpec(memory_space=pl.ANY)
    vmem = pl.BlockSpec(memory_space=pltpu.VMEM)
    n_cut = 4
    split = lambda w: v((2, w.shape[0] // 2, w.shape[1]), bf)
    scratch = [
        v(pre_gain.shape, f32), pltpu.SMEM(bias.shape, f32), pltpu.SMEM(sinks.shape, f32),
        v(sgain.shape, f32), v(wgain.shape, f32), v(post_gain.shape, f32),
        v((2, rows, feat_half), bf), v((2, rows, feat_half), bf),
        split(wqs), split(wks), split(wvs), split(wqw), split(wkw), split(wvw), v(wos.shape, bf), v(wow.shape, bf),
        v((3, rows, sw), f32),
        v((heads, rows + half, wide), bf), v((n_sp, rows + half, wide), bf),
        v((n_sp * rows, wide), bf),
        v((n_sp * rows, wide), f32), v((n_sp * rows, wide), f32),
        v((rows, sw), bf), v((rows, kvw_cols), bf), v((rows, kvw_cols), bf), v((rows, sw), bf),
        v((n_sp, half, wide), bf), v((heads, half, wide), bf),
        v((heads, rows, wide), bf), v((heads // 2, rows, wide), bf), v((rows, sw), f32), v((rows, sw), f32),
        v((2, rows, 128), f32), v((2, half, 128), f32), v((rows, feats), f32), v((rows, feats), f32),
        v((n_cut, half, feats // n_cut), bf), v((n_cut, half, feats // n_cut), bf),
        v((n_cut, half, feats // n_cut), bf), v((n_cut, half, feats // n_cut), bf),
        dma((14,)), dma((6,)), dma, dma, dma, dma((heads,)), dma((n_sp,)), dma((heads // 2,)),
        dma, dma, dma((n_sp,)), dma((heads,)), dma((heads,)), dma((heads // 2,)), dma((2,)), dma((2,)),
        dma((n_cut,)), dma((n_cut,)), dma((n_cut,)), dma((n_cut,)), pltpu.SemaphoreType.REGULAR, pltpu.SemaphoreType.REGULAR,
    ]
    return pl.pallas_call(
        functools.partial(kernel, n_sp),
        out_shape=pltpu.VMEM((half, feats), bf),
        in_specs=[anywhere] * len(args),
        out_specs=vmem,
        scratch_shapes=scratch,
        compiler_params=pltpu.CompilerParams(
            collective_id=0, has_side_effects=True, vmem_limit_bytes=60 * 1024 * 1024
        ),
        name="layer",
    )(*[pltpu.with_memory_space_constraint(a, pltpu.HBM) for a in args])


def passed_along(value, axis, steps):
    count = lax.axis_size(axis)
    initial, last = (max(0, -steps), min(count, count - steps))
    return lax.ppermute(value, axis, [(source, source + steps) for source in range(initial, last)])


def rounded(values):
    return lax.optimization_barrier(values.astype(jnp.bfloat16)).astype(jnp.float32)


def norm_rows(values, gain):
    stats = jnp.mean(values * values, axis=-1, keepdims=True)
    return values * lax.rsqrt(stats + EPS) * gain


def stick_block(queries, key_pair, head_bias, key_mask, carried):
    result, logsum = carried
    head_count = queries.shape[1]
    key_rows = key_pair[0].reshape(key_pair.shape[1], head_count, HEAD_DIM)
    values = key_pair[1].reshape(key_pair.shape[1], head_count, HEAD_DIM)
    scores = jnp.einsum(
        "thd,shd->hts", queries, key_rows, preferred_element_type=jnp.float32
    ) * HEAD_DIM ** (-0.5)
    scores = scores + head_bias[:, None, None]
    usable = key_mask[None]
    log_keep = jnp.where(usable, jax.nn.log_sigmoid(-scores), 0.0)
    suffix = lax.cumsum(log_keep, axis=2, reverse=True) - log_keep
    stick_weights = jnp.where(
        usable, jnp.exp(jax.nn.log_sigmoid(scores) + suffix + logsum[:, :, None]), 0.0
    )
    stick_weights = stick_weights.astype(jnp.bfloat16)
    result = result + jnp.einsum(
        "hts,shd->htd", stick_weights, values, preferred_element_type=jnp.float32
    )
    logsum = logsum + jnp.sum(log_keep, axis=2)
    return (result, logsum)


def by_collectives(
    tokens,
    pre_gain,
    w_query_stick,
    w_key_stick,
    w_value_stick,
    w_query_window,
    w_key_window,
    w_value_window,
    stick_bias,
    sinks,
    stick_gain,
    window_gain,
    w_out_stick,
    w_out_window,
    post_gain,
):
    gathered = lax.all_gather(tokens, "tp", axis=1, tiled=True)
    normed = norm_rows(gathered.astype(jnp.float32), pre_gain).astype(jnp.bfloat16)

    def project(weight):
        return jnp.dot(normed, weight, preferred_element_type=jnp.float32).astype(jnp.bfloat16)

    tok_rows = normed.shape[0]
    dev_index = lax.axis_index("sp")
    dev_count = lax.axis_size("sp")
    query_stick = project(w_query_stick)
    stick_heads = query_stick.shape[1] // HEAD_DIM
    queries = query_stick.reshape(tok_rows, stick_heads, HEAD_DIM)
    own_pair = jnp.stack([project(w_key_stick), project(w_value_stick)])
    pair_width = own_pair.shape[2]
    positions = jnp.arange(tok_rows, dtype=jnp.int32)
    initial = (
        jnp.zeros((stick_heads, tok_rows, HEAD_DIM), jnp.float32),
        jnp.zeros((stick_heads, tok_rows), jnp.float32),
    )
    collected = own_pair[None]
    for section_index in range(dev_count.bit_length() - 1):
        arrived = passed_along(collected, "sp", 2**section_index)
        collected = jnp.concatenate([arrived, collected], axis=0)
    per_group = min(dev_count, 8)
    group_count = dev_count // per_group
    grouped = collected.reshape(group_count, per_group, 2, tok_rows, pair_width)
    grouped = grouped.transpose(0, 2, 1, 3, 4).reshape(
        group_count, 2, per_group * tok_rows, pair_width
    )
    first_source = dev_index - (dev_count - 1)
    group_starts = (first_source + jnp.arange(group_count, dtype=jnp.int32) * per_group) * tok_rows
    query_pos = dev_index * tok_rows + positions
    span_offs = jnp.arange(per_group * tok_rows, dtype=jnp.int32)

    def visit_group(carried, inputs):
        key_pair, start_pos = inputs
        key_pos = start_pos + span_offs
        key_mask = (key_pos[None, :] >= 0) & (key_pos[None, :] < query_pos[:, None])
        return (stick_block(queries, key_pair, stick_bias, key_mask, carried), None)

    (stick_sum, _), _ = lax.scan(visit_group, initial, (grouped, group_starts), reverse=True)
    stick_out = (
        stick_sum.transpose(1, 0, 2).reshape(tok_rows, stick_heads * HEAD_DIM).astype(jnp.bfloat16)
    )
    query_window = project(w_query_window)
    window_pair = jnp.stack([project(w_key_window), project(w_value_window)])
    kv_heads = window_pair.shape[2] // HEAD_DIM
    previous = passed_along(window_pair, "sp", 1)
    extended = jnp.concatenate([previous, window_pair], axis=1)
    block_count = tok_rows // WINDOW
    extended = extended.reshape(2, block_count + 1, WINDOW, kv_heads, HEAD_DIM)
    banded = jnp.concatenate([extended[:, :-1], extended[:, 1:]], axis=2)
    q_blocks = query_window.reshape(block_count, WINDOW, kv_heads, GROUP, HEAD_DIM)
    logits = jnp.einsum(
        "nqhgd,nchd->nhgqc", q_blocks, banded[0], preferred_element_type=jnp.float32
    ) * HEAD_DIM ** (-0.5)
    query_offs = jnp.arange(WINDOW, dtype=jnp.int32)[:, None]
    key_offs = jnp.arange(2 * WINDOW, dtype=jnp.int32)[None, :]
    distance = query_offs + WINDOW - key_offs
    key_pos = (
        dev_index * tok_rows
        + jnp.arange(block_count, dtype=jnp.int32)[:, None] * WINDOW
        - WINDOW
        + key_offs
    )
    usable = ((distance >= 0) & (distance < WINDOW))[None] & (key_pos >= 0)[:, None, :]
    logits = jnp.where(usable[:, None, None], logits, -jnp.inf)
    sink_logit = sinks.reshape(kv_heads, GROUP)[None, :, :, None, None]
    row_top = jnp.maximum(jnp.max(logits, axis=-1, keepdims=True), sink_logit)
    weights_exp = jnp.exp(logits - row_top)
    normalizer = jnp.sum(weights_exp, axis=-1, keepdims=True) + jnp.exp(sink_logit - row_top)
    window_weights = (weights_exp / normalizer).astype(jnp.bfloat16)
    window_sum = jnp.einsum(
        "nhgqc,nchd->nqhgd", window_weights, banded[1], preferred_element_type=jnp.float32
    )
    window_out = window_sum.reshape(tok_rows, query_window.shape[1]).astype(jnp.bfloat16)
    stick_float = stick_out.astype(jnp.float32)
    window_float = window_out.astype(jnp.float32)
    squares = lax.psum(
        (jnp.sum(stick_float * stick_float, axis=1), jnp.sum(window_float * window_float, axis=1)),
        "tp",
    )
    stick_normed = (
        stick_float * lax.rsqrt(squares[0][:, None] / (stick_gain.shape[0] * lax.axis_size("tp")) + EPS) * stick_gain
    ).astype(jnp.bfloat16)
    window_normed = (
        window_float * lax.rsqrt(squares[1][:, None] / (window_gain.shape[0] * lax.axis_size("tp")) + EPS) * window_gain
    ).astype(jnp.bfloat16)
    total = jnp.dot(stick_normed, w_out_stick, preferred_element_type=jnp.float32)
    combined = lax.psum_scatter(
        (total + jnp.dot(window_normed, w_out_window, preferred_element_type=jnp.float32)).astype(
            jnp.bfloat16
        ),
        "tp",
        scatter_dimension=0,
        tiled=True,
    ).astype(jnp.float32)
    combined = rounded(combined)
    return norm_rows(combined, post_gain).astype(jnp.bfloat16)


def solution(mesh):
    in_specs = (
        P("sp", "tp"),
        P(),
        P(None, "tp"),
        P(None, "tp"),
        P(None, "tp"),
        P(None, "tp"),
        P(None, "tp"),
        P(None, "tp"),
        P("tp"),
        P("tp"),
        P("tp"),
        P("tp"),
        P("tp", None),
        P("tp", None),
        P(),
    )
    n_sp, n_tp = mesh.shape["sp"], mesh.shape["tp"]

    def shards(*args):
        heads = args[2].shape[1] // HEAD_DIM
        if n_tp == 2 and n_tp * heads == n_sp and args[0].shape[0] == WINDOW and heads == 4 * TILE_BLOCKS:
            return one_kernel(n_sp, *args)
        return by_collectives(*args)

    return jax.shard_map(
        shards,
        mesh=mesh,
        in_specs=in_specs,
        out_specs=P(("sp", "tp"), None),
        check_vma=False,
    )
```
